32 devices in a mesh: grp: 2 (over x), tp: 4 (over z), dp: 4 (over y, core).
Axes of the slice: x: 2, y: 2, z: 4, core: 2. Of those that a mesh axis runs over, the one named last changes fastest.
Arguments:
- tokens: bfloat16 [8, 4, 4096], P(('grp', 'tp'), None, 'dp'), parts along dimension 0, may hold values from -6 to 6
- lengths: int32 [8], P('grp'), parts along dimension 0, may hold values from 1 to 4, 8 in all
- norm_gain: float32 [2, 4096], P(None, 'dp'), may hold values from 0.1 to 1.9
- input_weight: bfloat16 [2, 4096, 8192], P(None, 'dp', 'tp'), may hold values from -0.09375 to 0.09375
- gate_weight: bfloat16 [2, 4096, 8192], P(None, 'dp', 'tp'), may hold values from -0.09375 to 0.09375
- decay_rate: float32 [2, 512, 64], P(None, 'tp'), may hold values from 0.05 to 2
- frequency: float32 [2, 512, 64], P(None, 'tp'), may hold values from 0 to 4
- log_step: float32 [2, 512], P(None, 'tp'), may hold values from -2.3 to 0
- input_map: bfloat16 [2, 512, 16, 128], P(None, 'tp'), may hold values from -1 to 1
- readout_map: bfloat16 [2, 512, 16, 128], P(None, 'tp'), may hold values from -0.5 to 0.5
- skip_weight: bfloat16 [2, 8192], P(None, 'tp'), may hold values from -4 to 4
- out_weight: bfloat16 [2, 8192, 4096], P(None, 'tp', 'dp'), may hold values from -0.0625 to 0.0625
- state: float32 [2, 8, 512, 128], P(None, ('grp', 'dp'), 'tp'), parts along dimension 1, may hold values from -5 to 5
Outputs:
- mixed: bfloat16 [8, 4, 4096], P(('grp', 'tp'), None, 'dp'), parts along dimension 0
- new_state: float32 [2, 8, 512, 128], P(None, ('grp', 'dp'), 'tp'), parts along dimension 1
The draws below stay inside these ranges and needn't reach their ends.
There are 2 independent parts, one for each index of `grp`. The reference program is written for one: setup_inputs(seed, part) draws one part's arguments, and reference() takes and returns one part's arrays. A program takes and returns all parts, laid end to end along the dimension named above; an argument that names none is the same for every part. Nothing has to cross between parts.
Inputs may be any that keep to these rules, and one draw needn't show every extreme that they name: `lengths`: the number of live new positions of each sequence; positions beyond it take no part.
All inputs are finite; a program needn't handle non-finite values.
Results may differ from the reference program's by a relative error of at most 0.023.
Values may be sent and summed in bfloat16 or wider, within the bound.
No kernel may reach another device: no remote copies, remote signals or barrier semaphores. Data moves between devices by JAX's collectives and lax.ppermute only.
A program may use at most 64 MiB of HBM per device.

```python
import math
import jax
import jax.numpy as jnp
import numpy as np
from jax import lax

D = 4096
E = 8192
S5_IN = 16
P_SIZE = 64
NEW = 4
LAYERS = 2
GROUPS = 512
SEQS = 4


def shard_levels(stream_key, extent, shards, low, high):
    def one(axis_at, parts):
        heights = jax.random.uniform(jax.random.fold_in(jax.random.fold_in(stream_key, 6), axis_at), (parts,), jnp.float32, low / len(shards), high / len(shards))
        return jnp.repeat(jnp.exp(heights), extent[axis_at] // parts).reshape((-1,) + (1,) * (len(extent) - axis_at - 1))

    factor_of = one(*shards[0])
    for cut in shards[1:]:
        factor_of = factor_of * one(*cut)
    return factor_of


def profile(count, total, limit, slope):
    portions = [(1 << 20) // math.isqrt(grade ** slope) + 1 for grade in range(2, count + 1)]
    rest, holding = total - limit - (count - 1), [1] * (count - 1)
    while rest > 0:
        movable = [i for i in range(count - 1) if holding[i] < limit]
        pool, budget = sum([portions[i] for i in movable]), rest
        for i in movable:
            extra = min(limit - holding[i], max(1, budget * portions[i] // pool), rest)
            holding[i] = holding[i] + extra
            rest = rest - extra
    return np.array([limit] + holding)


def ragged(own_key, count, total, bound, lean):
    if count == 2:
        one = jax.random.randint(own_key, (), max(1, total - bound), min(bound, total - 1) + 1)
        return jnp.stack([one, total - one])
    sizes = jnp.asarray(profile(count, total, bound, lean), jnp.int32)
    pairs = (count - 1) // 2
    source_of, receiver = sizes[1:1 + 2 * pairs:2], sizes[2:2 + 2 * pairs:2]
    slack = jnp.minimum(source_of - 1, bound - receiver)
    shifted = jax.random.randint(jax.random.fold_in(own_key, 1), (pairs,), 0, 1 << 20) % (slack + 1)
    sizes = sizes.at[1:1 + 2 * pairs:2].set(source_of - shifted).at[2:2 + 2 * pairs:2].set(receiver + shifted)
    return sizes[jax.random.permutation(jax.random.fold_in(own_key, 2), count)]


def gaussian(own_key, extent, width, limit, split=(), held_as=jnp.bfloat16):
    drawn = jax.random.normal(own_key, extent, jnp.float32) * width
    if len(split) > 0:
        drawn = shard_levels(own_key, extent, split, -0.22, 0.18) * drawn
    return jnp.clip(drawn, min=-limit, max=limit).astype(held_as)


def setup_inputs(seed: int = 0, part: int = 0) -> dict:
    splits = jax.random.split(jax.random.key(seed), 14)
    part_splits = jax.random.split(jax.random.fold_in(splits[13], part), 14)
    return {
        "tokens": gaussian(part_splits[0], (SEQS, NEW, D), 1.0, 6.0, ((0, 4), (2, 4))),
        "lengths": ragged(part_splits[1], SEQS, 2 * SEQS, NEW, 2).astype(jnp.int32),
        "norm_gain": jnp.clip(1.0 + 0.18 * jax.random.normal(splits[2], (LAYERS, D), jnp.float32), 0.1, 1.9),
        "input_weight": gaussian(splits[3], (LAYERS, D, E), D ** -0.5, 0.09375, ((1, 4), (2, 4))),
        "gate_weight": gaussian(splits[4], (LAYERS, D, E), D ** -0.5, 0.09375, ((1, 4), (2, 4))),
        "decay_rate": jnp.clip(jnp.exp(math.log(2.0) - 3.6888794 * jax.random.uniform(splits[5], (LAYERS, GROUPS, P_SIZE), jnp.float32) ** shard_levels(splits[5], (LAYERS, GROUPS, P_SIZE), ((1, 4),), -0.2, 0.2)), 0.05, 2.0),
        "frequency": jnp.clip(4.0 * jax.random.uniform(splits[6], (LAYERS, GROUPS, P_SIZE), jnp.float32) ** shard_levels(splits[6], (LAYERS, GROUPS, P_SIZE), ((1, 4),), -0.2, 0.2), 0.0, 4.0),
        "log_step": jnp.clip(-2.3 + 2.3 * jax.random.uniform(splits[7], (LAYERS, GROUPS), jnp.float32) ** shard_levels(splits[7], (LAYERS, GROUPS), ((1, 4),), -0.2, 0.2), -2.3, 0.0),
        "input_map": gaussian(splits[8], (LAYERS, GROUPS, S5_IN, 2 * P_SIZE), (2 * S5_IN) ** -0.5, 1.0, ((1, 4),)),
        "readout_map": gaussian(splits[9], (LAYERS, GROUPS, S5_IN, 2 * P_SIZE), (2 * P_SIZE) ** -0.5, 0.5, ((1, 4),)),
        "skip_weight": gaussian(splits[10], (LAYERS, E), 1.0, 4.0, ((1, 4),)),
        "out_weight": gaussian(splits[11], (LAYERS, E, D), E ** -0.5, 0.0625, ((1, 4), (2, 4))),
        "state": gaussian(part_splits[12], (LAYERS, SEQS, GROUPS, 2 * P_SIZE), 0.7, 5.0, ((1, 4), (2, 4)), jnp.float32),
    }


epsilon = 1e-06

def advance_state(drive_value, gate_value, carried, alive_mask, decay_rate, frequency, log_step, input_map, readout_map, skip_row):
    seq_count, new_count, inner_width = drive_value.shape
    group_count = inner_width // S5_IN
    state_half = carried.shape[-1] // 2
    step_size = jnp.exp(log_step)[:, None]
    magnitude = jnp.exp(-decay_rate * step_size)
    turn_angle = frequency * step_size
    decay_real = magnitude * jnp.cos(turn_angle)
    decay_imag = magnitude * jnp.sin(turn_angle)
    denominator = decay_rate * decay_rate + frequency * frequency
    coeff_real = (-(decay_real - 1.0) * decay_rate + decay_imag * frequency) / denominator
    coeff_imag = (-decay_imag * decay_rate - (decay_real - 1.0) * frequency) / denominator
    map_real = input_map[..., :state_half].astype(jnp.float32)
    map_imag = input_map[..., state_half:].astype(jnp.float32)
    coupled = jnp.concatenate([coeff_real[:, None, :] * map_real - coeff_imag[:, None, :] * map_imag, coeff_real[:, None, :] * map_imag + coeff_imag[:, None, :] * map_real], axis=-1)
    inputs = drive_value.astype(jnp.float32).reshape(seq_count, new_count, group_count, S5_IN)
    pushed = jnp.einsum('stgi,giq->stgq', inputs, coupled, precision=lax.Precision.HIGHEST)
    real_state = carried[..., :state_half]
    imag_state = carried[..., state_half:]
    history = []
    for position in range(new_count):
        keep = alive_mask[:, position][:, None, None] > 0.5
        next_real = decay_real * real_state - decay_imag * imag_state + pushed[:, position, :, :state_half]
        next_imag = decay_real * imag_state + decay_imag * real_state + pushed[:, position, :, state_half:]
        real_state = jnp.where(keep, next_real, real_state)
        imag_state = jnp.where(keep, next_imag, imag_state)
        history.append(jnp.concatenate([real_state, -imag_state], axis=-1))
    stacked = jnp.stack(history, axis=1)
    readout = jnp.einsum('stgq,giq->stgi', stacked, readout_map.astype(jnp.float32), precision=lax.Precision.HIGHEST)
    readout = readout.reshape(seq_count, new_count, inner_width)
    response = readout + skip_row.astype(jnp.float32) * inputs.reshape(seq_count, new_count, inner_width)
    branch = jax.nn.gelu(response) * jax.nn.silu(gate_value.astype(jnp.float32)) * alive_mask[:, :, None]
    return (jnp.concatenate([real_state, imag_state], axis=-1), branch.astype(jnp.bfloat16))

def reference(tokens, lengths, norm_gain, input_weight, gate_weight, decay_rate, frequency, log_step, input_map, readout_map, skip_weight, out_weight, state):
    seq_count, new_count, model_width = tokens.shape
    positions = lax.broadcasted_iota(jnp.int32, (seq_count, new_count), 1)
    alive_mask = (positions < lengths[:, None]).astype(jnp.float32)
    current = tokens
    states = []
    for layer_index in range(LAYERS):
        flattened = current.reshape(seq_count * new_count, model_width).astype(jnp.float32)
        inverse = lax.rsqrt(lax.optimization_barrier(jnp.mean(flattened * flattened, axis=1)) + epsilon)[:, None]
        scaled = (flattened * norm_gain[layer_index][None, :]).astype(jnp.bfloat16)
        drive_value = (inverse * jnp.dot(scaled, input_weight[layer_index], preferred_element_type=jnp.float32)).astype(jnp.bfloat16)
        gate_value = (inverse * jnp.dot(scaled, gate_weight[layer_index], preferred_element_type=jnp.float32)).astype(jnp.bfloat16)
        inner_width = drive_value.shape[1]
        next_state, branch = advance_state(drive_value.reshape(seq_count, new_count, inner_width), gate_value.reshape(seq_count, new_count, inner_width), state[layer_index], alive_mask, decay_rate[layer_index], frequency[layer_index], log_step[layer_index], input_map[layer_index], readout_map[layer_index], skip_weight[layer_index])
        states.append(next_state)
        projected = jnp.dot(branch.reshape(seq_count * new_count, inner_width), out_weight[layer_index], preferred_element_type=jnp.float32)
        current = (flattened + projected).astype(jnp.bfloat16).reshape(tokens.shape)
    return (current, jnp.stack(states))
```

```python
import jax
import jax.numpy as jnp
from jax import lax
from jax.sharding import PartitionSpec as P

D = 4096
S5_IN = 16
LAYERS = 2


epsilon = 1e-06


def advance_state(
    drive_value,
    gate_value,
    carried,
    alive_mask,
    decay_rate,
    frequency,
    log_step,
    input_map,
    readout_map,
    skip_row,
):
    seq_count, new_count, inner_width = drive_value.shape
    group_count = inner_width // S5_IN
    state_half = carried.shape[-1] // 2
    step_size = jnp.exp(log_step)[:, None]
    magnitude = jnp.exp(-decay_rate * step_size)
    turn_angle = frequency * step_size
    decay_real = magnitude * jnp.cos(turn_angle)
    decay_imag = magnitude * jnp.sin(turn_angle)
    denominator = decay_rate * decay_rate + frequency * frequency
    coeff_real = (-(decay_real - 1.0) * decay_rate + decay_imag * frequency) / denominator
    coeff_imag = (-decay_imag * decay_rate - (decay_real - 1.0) * frequency) / denominator
    map_real = input_map[..., :state_half].astype(jnp.float32)
    map_imag = input_map[..., state_half:].astype(jnp.float32)
    coupled = jnp.concatenate(
        [
            coeff_real[:, None, :] * map_real - coeff_imag[:, None, :] * map_imag,
            coeff_real[:, None, :] * map_imag + coeff_imag[:, None, :] * map_real,
        ],
        axis=-1,
    )
    inputs = drive_value.astype(jnp.float32).reshape(seq_count, new_count, group_count, S5_IN)
    pushed = jnp.einsum("stgi,giq->stgq", inputs, coupled, precision=lax.Precision.HIGHEST)
    real_state = carried[..., :state_half]
    imag_state = carried[..., state_half:]
    history = []
    for position in range(new_count):
        keep = alive_mask[:, position][:, None, None] > 0.5
        next_real = (
            decay_real * real_state - decay_imag * imag_state + pushed[:, position, :, :state_half]
        )
        next_imag = (
            decay_real * imag_state + decay_imag * real_state + pushed[:, position, :, state_half:]
        )
        real_state = jnp.where(keep, next_real, real_state)
        imag_state = jnp.where(keep, next_imag, imag_state)
        history.append(jnp.concatenate([real_state, -imag_state], axis=-1))
    stacked = jnp.stack(history, axis=1)
    readout = jnp.einsum(
        "stgq,giq->stgi", stacked, readout_map.astype(jnp.float32), precision=lax.Precision.HIGHEST
    )
    readout = readout.reshape(seq_count, new_count, inner_width)
    response = readout + skip_row.astype(jnp.float32) * inputs.reshape(
        seq_count, new_count, inner_width
    )
    branch = (
        jax.nn.gelu(response) * jax.nn.silu(gate_value.astype(jnp.float32)) * alive_mask[:, :, None]
    )
    return (jnp.concatenate([real_state, imag_state], axis=-1), branch.astype(jnp.bfloat16))


def direct(size):
    return 1 < size <= 8 and size & (size - 1) == 0


def swap(value, axis, distance, size):
    return lax.ppermute(value, axis, [(i, i ^ distance) for i in range(size)])


def gather_rows(block, axis, size):
    if not direct(size):
        return lax.all_gather(block, axis, axis=0, tiled=True)
    index = lax.axis_index(axis)
    slots = jnp.stack([block] + [swap(block, axis, k, size) for k in range(1, size)])
    ordered = [lax.dynamic_index_in_dim(slots, index ^ s, 0, keepdims=False) for s in range(size)]
    return jnp.concatenate(ordered, axis=0)


def exchange_rows(value, axis, size):
    index = lax.axis_index(axis)
    rows = value.shape[0] // size
    blocks = [
        lax.dynamic_slice_in_dim(value, (index ^ k) * rows, rows, 0) for k in range(size)
    ]
    return [blocks[0]] + [swap(blocks[k], axis, k, size) for k in range(1, size)]


def split_three(value):
    pieces = []
    for _ in range(3):
        piece = lax.reduce_precision(value, 8, 7)
        pieces.append(piece.astype(jnp.bfloat16))
        value = value - piece
    return pieces


def scatter_projections(part_drive, part_gate, squares, axis, size):
    index = lax.axis_index(axis)
    width = part_drive.shape[1]
    rows = part_drive.shape[0] // size
    if not direct(size):
        total = lax.psum(squares, axis)
        own = lax.dynamic_slice_in_dim(total, index * rows, rows, 0)
        drive, gate = (
            lax.psum_scatter(
                part.astype(jnp.bfloat16), axis, scatter_dimension=0, tiled=True
            ).astype(jnp.float32)
            for part in (part_drive, part_gate)
        )
        return drive, gate, own
    extra = jnp.stack(split_three(squares), axis=1)
    extra = jnp.pad(extra, ((0, 0), (0, 128 - extra.shape[1])))
    message = jnp.concatenate(
        [part_drive.astype(jnp.bfloat16), part_gate.astype(jnp.bfloat16), extra], axis=1
    )
    total = sum(part.astype(jnp.float32) for part in exchange_rows(message, axis, size))
    own = jnp.sum(total[:, 2 * width :], axis=1)
    return total[:, :width], total[:, width : 2 * width], own


def body(
    tokens,
    lengths,
    norm_gain,
    input_weight,
    gate_weight,
    decay_rate,
    frequency,
    log_step,
    input_map,
    readout_map,
    skip_weight,
    out_weight,
    state,
):
    own_seqs = state.shape[1]
    block_seqs, new_count, feature_count = tokens.shape
    all_seqs = lengths.shape[0]
    inner_width = input_weight.shape[2]
    dp_index = lax.axis_index("dp")
    tp_index = lax.axis_index("tp")
    dp_size = lax.axis_size("dp")
    tp_size = lax.axis_size("tp")
    positions = lax.broadcasted_iota(jnp.int32, (all_seqs, new_count), 1)
    alive_all = (positions < lengths[:, None]).astype(jnp.float32)
    alive_own = lax.dynamic_slice_in_dim(alive_all, dp_index * own_seqs, own_seqs, 0)
    own_rows = own_seqs * new_count
    block_count = block_seqs * new_count
    states = []
    gathered = gather_rows(tokens.reshape(block_count, feature_count), "tp", tp_size)
    for layer_index in range(LAYERS):
        flattened = gathered.astype(jnp.float32)
        scaled = (flattened * norm_gain[layer_index][None, :]).astype(jnp.bfloat16)
        partial_squares = jnp.sum(flattened * flattened, axis=1)
        part_drive = jnp.dot(scaled, input_weight[layer_index], preferred_element_type=jnp.float32)
        part_gate = jnp.dot(scaled, gate_weight[layer_index], preferred_element_type=jnp.float32)
        summed_drive, summed_gate, own_squares = scatter_projections(
            part_drive, part_gate, partial_squares, "dp", dp_size
        )
        inverse = lax.rsqrt(own_squares / D + epsilon)[:, None]
        drive_value = (
            (inverse * summed_drive).astype(jnp.bfloat16).reshape(own_seqs, new_count, inner_width)
        )
        gate_value = (
            (inverse * summed_gate).astype(jnp.bfloat16).reshape(own_seqs, new_count, inner_width)
        )
        next_state, branch = advance_state(
            drive_value,
            gate_value,
            state[layer_index],
            alive_own,
            decay_rate[layer_index],
            frequency[layer_index],
            log_step[layer_index],
            input_map[layer_index],
            readout_map[layer_index],
            skip_weight[layer_index],
        )
        states.append(next_state)
        weight_now = out_weight[layer_index]
        projected = jnp.dot(
            gather_rows(branch.reshape(own_rows, inner_width), "dp", dp_size),
            weight_now,
            preferred_element_type=jnp.float32,
        ).astype(jnp.bfloat16)
        last = layer_index == LAYERS - 1
        if direct(tp_size) and not last:
            parts = [projected] + [swap(projected, "tp", k, tp_size) for k in range(1, tp_size)]
            total = sum(part.astype(jnp.float32) for part in parts)
            gathered = (flattened + total).astype(jnp.bfloat16)
            continue
        if direct(tp_size):
            parts = exchange_rows(projected, "tp", tp_size)
            branch_sum = sum(part.astype(jnp.float32) for part in parts)
        else:
            branch_sum = lax.psum_scatter(
                projected, "tp", scatter_dimension=0, tiled=True
            ).astype(jnp.float32)
        own_base = lax.dynamic_slice_in_dim(flattened, tp_index * block_count, block_count, 0)
        own_block = (own_base + branch_sum).astype(jnp.bfloat16)
        if not last:
            gathered = lax.all_gather(own_block, "tp", axis=0, tiled=True)
    own_block = own_block.reshape(tokens.shape)
    return (own_block, jnp.stack(states))


def solution(mesh):
    return jax.shard_map(
        body,
        mesh=mesh,
        in_specs=(
            P(("grp", "tp"), None, "dp"),
            P("grp"),
            P(None, "dp"),
            P(None, "dp", "tp"),
            P(None, "dp", "tp"),
            P(None, "tp", None),
            P(None, "tp", None),
            P(None, "tp"),
            P(None, "tp", None, None),
            P(None, "tp", None, None),
            P(None, "tp"),
            P(None, "tp", "dp"),
            P(None, ("grp", "dp"), "tp", None),
        ),
        out_specs=(P(("grp", "tp"), None, "dp"), P(None, ("grp", "dp"), "tp", None)),
        check_vma=False,
    )
```

```python
import functools

import jax
import jax.numpy as jnp
from jax import lax
from jax.experimental import pallas as pl
from jax.experimental.pallas import tpu as pltpu
from jax.sharding import PartitionSpec as P

D = 4096
S5_IN = 16
LAYERS = 2


epsilon = 1e-06


def advance_state(
    drive_value,
    gate_value,
    carried,
    alive_mask,
    decay_rate,
    frequency,
    log_step,
    input_map,
    readout_map,
    skip_row,
):
    seq_count, new_count, inner_width = drive_value.shape
    group_count = inner_width // S5_IN
    state_half = carried.shape[-1] // 2
    step_size = jnp.exp(log_step)[:, None]
    magnitude = jnp.exp(-decay_rate * step_size)
    turn_angle = frequency * step_size
    decay_real = magnitude * jnp.cos(turn_angle)
    decay_imag = magnitude * jnp.sin(turn_angle)
    denominator = decay_rate * decay_rate + frequency * frequency
    coeff_real = (-(decay_real - 1.0) * decay_rate + decay_imag * frequency) / denominator
    coeff_imag = (-decay_imag * decay_rate - (decay_real - 1.0) * frequency) / denominator
    map_real = input_map[..., :state_half].astype(jnp.float32)
    map_imag = input_map[..., state_half:].astype(jnp.float32)
    coupled = jnp.concatenate(
        [
            coeff_real[:, None, :] * map_real - coeff_imag[:, None, :] * map_imag,
            coeff_real[:, None, :] * map_imag + coeff_imag[:, None, :] * map_real,
        ],
        axis=-1,
    )
    inputs = drive_value.astype(jnp.float32).reshape(seq_count, new_count, group_count, S5_IN)
    pushed = jnp.einsum("stgi,giq->stgq", inputs, coupled, precision=lax.Precision.HIGHEST)
    real_state = carried[..., :state_half]
    imag_state = carried[..., state_half:]
    history = []
    for position in range(new_count):
        keep = alive_mask[:, position][:, None, None] > 0.5
        next_real = (
            decay_real * real_state - decay_imag * imag_state + pushed[:, position, :, :state_half]
        )
        next_imag = (
            decay_real * imag_state + decay_imag * real_state + pushed[:, position, :, state_half:]
        )
        real_state = jnp.where(keep, next_real, real_state)
        imag_state = jnp.where(keep, next_imag, imag_state)
        history.append(jnp.concatenate([real_state, -imag_state], axis=-1))
    stacked = jnp.stack(history, axis=1)
    readout = jnp.einsum(
        "stgq,giq->stgi", stacked, readout_map.astype(jnp.float32), precision=lax.Precision.HIGHEST
    )
    readout = readout.reshape(seq_count, new_count, inner_width)
    response = readout + skip_row.astype(jnp.float32) * inputs.reshape(
        seq_count, new_count, inner_width
    )
    branch = (
        jax.nn.gelu(response) * jax.nn.silu(gate_value.astype(jnp.float32)) * alive_mask[:, :, None]
    )
    return (jnp.concatenate([real_state, imag_state], axis=-1), branch.astype(jnp.bfloat16))


def direct(size):
    return 1 < size <= 8 and size & (size - 1) == 0


def swap(value, axis, distance, size):
    return lax.ppermute(value, axis, [(i, i ^ distance) for i in range(size)])


def gather_rows(block, axis, size):
    if not direct(size):
        return lax.all_gather(block, axis, axis=0, tiled=True)
    index = lax.axis_index(axis)
    slots = jnp.stack([block] + [swap(block, axis, k, size) for k in range(1, size)])
    ordered = [lax.dynamic_index_in_dim(slots, index ^ s, 0, keepdims=False) for s in range(size)]
    return jnp.concatenate(ordered, axis=0)


def exchange_rows(value, axis, size):
    index = lax.axis_index(axis)
    rows = value.shape[0] // size
    blocks = [
        lax.dynamic_slice_in_dim(value, (index ^ k) * rows, rows, 0) for k in range(size)
    ]
    return [blocks[0]] + [swap(blocks[k], axis, k, size) for k in range(1, size)]


def split_three(value):
    pieces = []
    for _ in range(3):
        piece = lax.reduce_precision(value, 8, 7)
        pieces.append(piece.astype(jnp.bfloat16))
        value = value - piece
    return pieces


def scatter_projections(part_drive, part_gate, squares, axis, size):
    index = lax.axis_index(axis)
    width = part_drive.shape[1]
    rows = part_drive.shape[0] // size
    if not direct(size):
        total = lax.psum(squares, axis)
        own = lax.dynamic_slice_in_dim(total, index * rows, rows, 0)
        drive, gate = (
            lax.psum_scatter(
                part.astype(jnp.bfloat16), axis, scatter_dimension=0, tiled=True
            ).astype(jnp.float32)
            for part in (part_drive, part_gate)
        )
        return drive, gate, own
    extra = jnp.stack(split_three(squares), axis=1)
    extra = jnp.pad(extra, ((0, 0), (0, 128 - extra.shape[1])))
    message = jnp.concatenate(
        [part_drive.astype(jnp.bfloat16), part_gate.astype(jnp.bfloat16), extra], axis=1
    )
    total = sum(part.astype(jnp.float32) for part in exchange_rows(message, axis, size))
    own = jnp.sum(total[:, 2 * width :], axis=1)
    return total[:, :width], total[:, width : 2 * width], own


def general_body(
    tokens,
    lengths,
    norm_gain,
    input_weight,
    gate_weight,
    decay_rate,
    frequency,
    log_step,
    input_map,
    readout_map,
    skip_weight,
    out_weight,
    state,
):
    own_seqs = state.shape[1]
    block_seqs, new_count, feature_count = tokens.shape
    all_seqs = lengths.shape[0]
    inner_width = input_weight.shape[2]
    dp_index = lax.axis_index("dp")
    tp_index = lax.axis_index("tp")
    dp_size = lax.axis_size("dp")
    tp_size = lax.axis_size("tp")
    positions = lax.broadcasted_iota(jnp.int32, (all_seqs, new_count), 1)
    alive_all = (positions < lengths[:, None]).astype(jnp.float32)
    alive_own = lax.dynamic_slice_in_dim(alive_all, dp_index * own_seqs, own_seqs, 0)
    own_rows = own_seqs * new_count
    block_count = block_seqs * new_count
    states = []
    gathered = gather_rows(tokens.reshape(block_count, feature_count), "tp", tp_size)
    for layer_index in range(LAYERS):
        flattened = gathered.astype(jnp.float32)
        scaled = (flattened * norm_gain[layer_index][None, :]).astype(jnp.bfloat16)
        partial_squares = jnp.sum(flattened * flattened, axis=1)
        part_drive = jnp.dot(scaled, input_weight[layer_index], preferred_element_type=jnp.float32)
        part_gate = jnp.dot(scaled, gate_weight[layer_index], preferred_element_type=jnp.float32)
        summed_drive, summed_gate, own_squares = scatter_projections(
            part_drive, part_gate, partial_squares, "dp", dp_size
        )
        inverse = lax.rsqrt(own_squares / D + epsilon)[:, None]
        drive_value = (
            (inverse * summed_drive).astype(jnp.bfloat16).reshape(own_seqs, new_count, inner_width)
        )
        gate_value = (
            (inverse * summed_gate).astype(jnp.bfloat16).reshape(own_seqs, new_count, inner_width)
        )
        next_state, branch = advance_state(
            drive_value,
            gate_value,
            state[layer_index],
            alive_own,
            decay_rate[layer_index],
            frequency[layer_index],
            log_step[layer_index],
            input_map[layer_index],
            readout_map[layer_index],
            skip_weight[layer_index],
        )
        states.append(next_state)
        weight_now = out_weight[layer_index]
        projected = jnp.dot(
            gather_rows(branch.reshape(own_rows, inner_width), "dp", dp_size),
            weight_now,
            preferred_element_type=jnp.float32,
        ).astype(jnp.bfloat16)
        last = layer_index == LAYERS - 1
        if direct(tp_size) and not last:
            parts = [projected] + [swap(projected, "tp", k, tp_size) for k in range(1, tp_size)]
            total = sum(part.astype(jnp.float32) for part in parts)
            gathered = (flattened + total).astype(jnp.bfloat16)
            continue
        if direct(tp_size):
            parts = exchange_rows(projected, "tp", tp_size)
            branch_sum = sum(part.astype(jnp.float32) for part in parts)
        else:
            branch_sum = lax.psum_scatter(
                projected, "tp", scatter_dimension=0, tiled=True
            ).astype(jnp.float32)
        own_base = lax.dynamic_slice_in_dim(flattened, tp_index * block_count, block_count, 0)
        own_block = (own_base + branch_sum).astype(jnp.bfloat16)
        if not last:
            gathered = lax.all_gather(own_block, "tp", axis=0, tiled=True)
    own_block = own_block.reshape(tokens.shape)
    return (own_block, jnp.stack(states))


LANES = 128
COST = 4000000
SUBLANES = 8
VMEM = pl.BlockSpec(memory_space=pltpu.VMEM)
HBM = pl.BlockSpec(memory_space=pltpu.MemorySpace.HBM)


def vmem_call(kernel, outs, *operands, in_specs=None, scratch=(), limit=8 << 20, cost=0):
    outs = [jax.ShapeDtypeStruct(shape, dtype) for shape, dtype in outs]
    in_specs = in_specs or [VMEM] * len(operands)
    operands = [
        pltpu.with_memory_space_constraint(operand, pltpu.MemorySpace.HBM) if spec is HBM else operand
        for spec, operand in zip(in_specs, operands)
    ]
    return pl.pallas_call(
        kernel,
        out_shape=outs,
        in_specs=in_specs,
        out_specs=[VMEM] * len(outs),
        scratch_shapes=list(scratch),
        compiler_params=pltpu.CompilerParams(vmem_limit_bytes=limit),
        cost_estimate=pl.CostEstimate(flops=cost, bytes_accessed=0, transcendentals=0) if cost else None,
    )(*operands)


def twice(value):
    return jnp.concatenate([value, value], axis=-1)


def halves(value):
    high = value.astype(jnp.bfloat16)
    low = (value - high.astype(jnp.float32)).astype(jnp.bfloat16)
    return high, low


def group_mask(dtype=jnp.float32):
    lane = lax.broadcasted_iota(jnp.int32, (SUBLANES, LANES), 1)
    row = lax.broadcasted_iota(jnp.int32, (SUBLANES, LANES), 0)
    return lane // S5_IN == row


def start_copies(sources, targets, semaphores):
    copies = [
        pltpu.make_async_copy(source, target, semaphores.at[i])
        for i, (source, target) in enumerate(zip(sources, targets))
    ]
    for copy in copies:
        copy.start()
    return copies


def wait_copies(copies):
    for copy in copies:
        copy.wait()


def parameter_step(decay, frequency, log_step, map_ref, real_ref, imag_ref, coupled_ref):
    half, groups = decay.shape
    step = jnp.exp(log_step)
    magnitude = jnp.exp(-decay * step)
    angle = frequency * step
    real = magnitude * jnp.cos(angle)
    imag = magnitude * jnp.sin(angle)
    denominator = decay * decay + frequency * frequency
    coeff_real = (imag * frequency - (real - 1.0) * decay) / denominator
    coeff_imag = (-imag * decay - (real - 1.0) * frequency) / denominator

    def across(first, second):
        return jnp.transpose(jnp.concatenate([first, second], axis=0))

    real_ref[...] = across(real, real)
    imag_ref[...] = across(-imag, imag)
    scale_real = across(coeff_real, coeff_real)
    scale_imag = across(-coeff_imag, coeff_imag)
    for chunk in range(groups // SUBLANES):
        rows = slice(chunk * SUBLANES, (chunk + 1) * SUBLANES)
        values = map_ref[rows].astype(jnp.float32).reshape(LANES, LANES)
        spread = [
            jnp.broadcast_to(s[rows][:, None, :], (SUBLANES, S5_IN, LANES)).reshape(LANES, LANES)
            for s in (scale_real, scale_imag)
        ]
        coupled = spread[0] * values + spread[1] * pltpu.roll(values, half, 1)
        high, low = halves(coupled)
        coupled_ref[chunk, :LANES] = high
        coupled_ref[chunk, LANES:] = low


def prepare_kernel(layer, decay_hbm, frequency_hbm, log_step_hbm, map_hbm, *refs):
    count = (len(refs) - 8) // 2
    sources, targets = refs[:count], refs[count : 2 * count]
    real_ref, imag_ref, coupled_ref = refs[2 * count : 2 * count + 3]
    decay, frequency, log_step, maps, semaphores = refs[2 * count + 3 :]
    small = start_copies(
        [decay_hbm.at[layer], frequency_hbm.at[layer], log_step_hbm, map_hbm.at[layer]],
        [decay, frequency, log_step, maps],
        semaphores.at[pl.ds(0, 4)],
    )
    large = start_copies(
        [source.at[layer] for source in sources], targets, semaphores.at[pl.ds(4, count)]
    )
    wait_copies(small)
    parameter_step(
        decay[...], frequency[...], log_step[layer : layer + 1], maps, real_ref, imag_ref, coupled_ref
    )
    wait_copies(large)


def prepare(layer, decay, frequency, log_step, input_map, projections, after=()):
    _, half, groups = decay.shape
    f32, bf16 = jnp.float32, jnp.bfloat16
    after = list(after)

    def kernel(*refs):
        prepare_kernel(layer, *refs[len(after) :])

    return vmem_call(
        kernel,
        [(p.shape[1:], bf16) for p in projections]
        + [((groups, LANES), f32)] * 2
        + [((groups // SUBLANES, 2 * LANES, LANES), bf16)],
        *after, decay, frequency, log_step, input_map, *projections,
        in_specs=[VMEM] * len(after) + [HBM] * (4 + len(projections)),
        scratch=[
            pltpu.VMEM((half, groups), f32),
            pltpu.VMEM((half, groups), f32),
            pltpu.VMEM(log_step.shape, f32),
            pltpu.VMEM(input_map.shape[1:], bf16),
            pltpu.SemaphoreType.DMA((4 + len(projections),)),
        ],
        cost=COST,
    )


def small_kernel(steps, lengths_hbm, *refs):
    count = (len(refs) - 3) // 2
    sources, targets = refs[:count], refs[count : 2 * count]
    live_ref, lengths, semaphores = refs[2 * count :]
    copies = start_copies(
        [lengths_hbm, *sources], [lengths, *targets], semaphores
    )
    copies[0].wait()
    length = lengths[lax.axis_index("dp")]
    place = lax.broadcasted_iota(jnp.int32, (steps * SUBLANES, LANES), 0) // SUBLANES
    live_ref[...] = (place < length).astype(jnp.float32)
    wait_copies(copies[1:])


def bring_small(steps, lengths, *arrays):
    return vmem_call(
        functools.partial(small_kernel, steps),
        [(a.shape, a.dtype) for a in arrays] + [((steps * SUBLANES, LANES), jnp.float32)],
        lengths, *arrays,
        in_specs=[HBM] * (1 + len(arrays)),
        scratch=[
            pltpu.SMEM(lengths.shape, jnp.int32),
            pltpu.SemaphoreType.DMA((1 + len(arrays),)),
        ],
        cost=COST,
    )


def bring_all_kernel(count, after, *refs):
    wait_copies(start_copies(refs[:count], refs[count : 2 * count], refs[-1]))


def bring_both(arrays, after):
    return vmem_call(
        functools.partial(bring_all_kernel, len(arrays)),
        [(a.shape, a.dtype) for a in arrays],
        after, *arrays,
        in_specs=[VMEM] + [HBM] * len(arrays),
        scratch=[pltpu.SemaphoreType.DMA((len(arrays),))],
        cost=COST,
    )


def swaps(values, axis, size):
    received = {}
    for k in reversed(range(1, size)):
        with jax.named_scope(f"k{k}"):
            value = values[k] if isinstance(values, (list, tuple)) else values
            received[k] = swap(value, axis, k, size)
    return [received[k] for k in range(1, size)]


def bring_kernel(layer, source, after, target, semaphores):
    wait_copies(start_copies([source.at[layer]], [target], semaphores))


def bring(layer, source, after):
    return vmem_call(
        functools.partial(bring_kernel, layer),
        [(source.shape[1:], source.dtype)],
        source, after,
        in_specs=[HBM, VMEM],
        scratch=[pltpu.SemaphoreType.DMA((1,))],
        cost=COST,
    )[0]


def project(layer, rows, gain_ref, drive_weight_ref, gate_weight_ref, message_refs):
    count = rows.shape[0] // len(message_refs)
    width = drive_weight_ref.shape[1]
    scaled = (rows * gain_ref[layer : layer + 1]).astype(jnp.bfloat16)
    squares = jnp.sum(rows * rows, axis=1, keepdims=True)
    lane = lax.broadcasted_iota(jnp.int32, (rows.shape[0], LANES), 1)
    extra = jnp.zeros((rows.shape[0], LANES), jnp.float32)
    for place in range(3):
        piece = squares.astype(jnp.bfloat16).astype(jnp.float32)
        extra = jnp.where(lane == place, piece, extra)
        squares = squares - piece
    step = min(width, 512)
    parts = [(2 * width, LANES, extra)]
    for base, weight_ref in ((0, drive_weight_ref), (width, gate_weight_ref)):
        for at in range(0, width, step):
            value = jnp.dot(
                scaled, weight_ref[:, at : at + step], preferred_element_type=jnp.float32
            )
            parts.append((base + at, step, value))
    for at, size, value in parts:
        for k, message_ref in enumerate(message_refs):
            block = value[k * count : (k + 1) * count]
            message_ref[:, at : at + size] = block.astype(jnp.bfloat16)


def pick(blocks, offset):
    bit = 1
    while bit < len(blocks):
        on = (offset & bit) != 0
        blocks = [jnp.where(on, blocks[k ^ bit], blocks[k]) for k in range(len(blocks))]
        bit *= 2
    return blocks


def own_offset():
    return lax.axis_index("dp") ^ lax.axis_index("tp")


def first_kernel(size, *refs):
    block_refs, (gain_ref, drive_ref, gate_ref) = refs[:size], refs[size : size + 3]
    message_refs, rows_ref = refs[size + 3 : -1], refs[-1]
    blocks = [ref[...].astype(jnp.float32).reshape(ref.shape[-2:]) for ref in block_refs]
    rows = jnp.concatenate(pick(blocks, own_offset()), axis=0)
    rows_ref[...] = rows
    project(0, rows, gain_ref, drive_ref, gate_ref, message_refs)


def next_kernel(size, layer, base_ref, *refs):
    part_refs, (gain_ref, drive_ref, gate_ref) = refs[:size], refs[size : size + 3]
    message_refs, rows_ref = refs[size + 3 : -1], refs[-1]
    rows = base_ref[...]
    rows = rows + sum(ref[...].astype(jnp.float32) for ref in part_refs)
    rows = rows.astype(jnp.bfloat16).astype(jnp.float32)
    rows_ref[...] = rows
    project(layer, rows, gain_ref, drive_ref, gate_ref, message_refs)


def state_kernel(size, layer, features, *refs):
    message_refs = refs[:size]
    live_ref, real_ref, imag_ref, coupled_ref, readout_ref, skip_ref, state_ref = refs[size:-2]
    branch_ref, next_ref = refs[-2:]
    steps = message_refs[0].shape[0]
    width = branch_ref.shape[1]
    half = LANES // 2
    total = sum(ref[...].astype(jnp.float32) for ref in message_refs)
    squares = jnp.sum(total[:, 2 * width :], axis=1, keepdims=True)
    inverse = lax.rsqrt(squares / features + epsilon)
    drive = (inverse * total[:, :width]).astype(jnp.bfloat16).astype(jnp.float32)
    gate = (inverse * total[:, width : 2 * width]).astype(jnp.bfloat16).astype(jnp.float32)
    live = live_ref[...]
    lane = lax.broadcasted_iota(jnp.int32, (SUBLANES, LANES), 1)
    row = lax.broadcasted_iota(jnp.int32, (SUBLANES, LANES), 0)
    own_group = group_mask()
    keeps = [live[t * SUBLANES : (t + 1) * SUBLANES] > 0.5 for t in range(steps)]
    live_rows = jnp.concatenate(
        [live[t * SUBLANES : t * SUBLANES + 1] for t in range(steps)], axis=0
    )
    sign = jnp.where(lane < half, 1.0, -1.0)
    for chunk in range(width // LANES):
        at = slice(chunk * LANES, (chunk + 1) * LANES)
        groups = slice(chunk * SUBLANES, (chunk + 1) * SUBLANES)
        fed = jnp.concatenate(
            [
                jnp.where(own_group, jnp.broadcast_to(drive[t : t + 1, at], (SUBLANES, LANES)), 0.0)
                for t in range(steps)
            ],
            axis=0,
        ).astype(jnp.bfloat16)
        pushed = jnp.dot(twice(fed), coupled_ref[chunk], preferred_element_type=jnp.float32)
        turned = pltpu.roll(pushed, half, 1)
        real, imag = real_ref[groups], imag_ref[groups]
        value = state_ref[layer, 0, groups]
        other = pltpu.roll(value, half, 1)
        history = []
        for t in range(steps):
            now = slice(t * SUBLANES, (t + 1) * SUBLANES)
            new_value = real * value + imag * other + pushed[now]
            new_other = real * other - imag * value + turned[now]
            value = jnp.where(keeps[t], new_value, value)
            other = jnp.where(keeps[t], new_other, other)
            history.append(value * sign)
        next_ref[groups] = value
        high, low = halves(jnp.concatenate(history, axis=0))
        seen = lax.dot_general(
            jnp.concatenate([high, low], axis=0),
            readout_ref[chunk],
            (((1,), (1,)), ((), ())),
            preferred_element_type=jnp.float32,
        )
        count = steps * SUBLANES
        seen = seen[:count] + seen[count:]
        read = jnp.concatenate(
            [
                jnp.sum(
                    jnp.where(own_group, seen[t * SUBLANES : (t + 1) * SUBLANES], 0.0),
                    axis=0,
                    keepdims=True,
                )
                for t in range(steps)
            ],
            axis=0,
        )
        response = read + skip_ref[layer : layer + 1, at].astype(jnp.float32) * drive[:, at]
        value = jax.nn.gelu(response) * jax.nn.silu(gate[:, at]) * live_rows
        branch_ref[:, at] = value.astype(jnp.bfloat16)


def output_kernel(size, *refs):
    branch_refs, weight_ref, out_ref = refs[:size], refs[size], refs[size + 1]
    rows = jnp.concatenate([ref[...].astype(jnp.float32) for ref in branch_refs], axis=0)
    out_ref[...] = jnp.dot(
        rows.astype(jnp.bfloat16), weight_ref[...], preferred_element_type=jnp.float32
    ).astype(jnp.bfloat16)


def last_output_kernel(size, *refs):
    branch_refs, weight_ref, base_ref = refs[:size], refs[size], refs[size + 1]
    out_refs = refs[size + 2 :]
    rows = jnp.concatenate([ref[...].astype(jnp.float32) for ref in branch_refs], axis=0)
    value = jnp.dot(rows.astype(jnp.bfloat16), weight_ref[...], preferred_element_type=jnp.float32)
    count = rows.shape[0] // size
    blocks = [value[k * count : (k + 1) * count] for k in range(size)]
    offset = own_offset()
    blocks = pick(blocks, offset)
    base = base_ref[...]
    bases = pick([base[k * count : (k + 1) * count] for k in range(size)], offset)
    out_refs[0][...] = bases[0] + blocks[0]
    for out_ref, block in zip(out_refs[1:], blocks[1:]):
        out_ref[...] = block.astype(jnp.bfloat16)


def final_kernel(own_ref, *refs):
    total = own_ref[...] + sum(ref[...].astype(jnp.float32) for ref in refs[:-1])
    refs[-1][0] = total.astype(jnp.bfloat16)


def fits(tokens, lengths, state, map_rows, dp_size, tp_size):
    whole_groups = state.shape[2] % LANES == 0 and state.shape[3] == LANES
    one_each = tokens.shape[0] == 1 and state.shape[1] == 1
    equal = dp_size == tp_size == lengths.shape[0]
    return direct(dp_size) and equal and one_each and whole_groups and map_rows == S5_IN


def direct_body(
    tokens,
    lengths,
    norm_gain,
    input_weight,
    gate_weight,
    decay_rate,
    frequency,
    log_step,
    input_map,
    readout_map,
    skip_weight,
    out_weight,
    state,
):
    size = lax.axis_size("dp")
    _, steps, features = tokens.shape
    inner = input_weight.shape[2]
    groups = state.shape[2]
    chunks = groups // SUBLANES
    count = size * steps
    bf16, f32 = jnp.bfloat16, jnp.float32
    message = [((steps, 2 * inner + LANES), bf16)] * size
    rows_shape = ((count, features), f32)
    projections = (input_weight, gate_weight)
    decay, frequency = (jnp.swapaxes(value, 1, 2) for value in (decay_rate, frequency))
    raw = (decay, frequency, log_step, input_map, projections)
    own = tokens.reshape(steps, features)
    with jax.named_scope("a"):
        pieces = swaps(own, "tp", size)
        own, gain, live = bring_small(steps, lengths, own, norm_gain)
        pieces = [own] + pieces
        *weights, real, imag, coupled = prepare(0, *raw)
    states = []
    for layer in range(LAYERS):
        if layer == 0:
            kernel, base = functools.partial(first_kernel, size), []
        else:
            kernel, base = functools.partial(next_kernel, size, layer), [rows]
        results = vmem_call(kernel, message + [rows_shape], *base, *pieces, gain, *weights)
        messages, rows = results[:size], results[size]
        with jax.named_scope(f"b{layer}"):
            arrived = [messages[0]] + swaps(messages, "dp", size)
            out_now = bring(layer, out_weight, messages[0])
            readout = bring(layer, readout_map, messages[0])
            if layer == 0:
                state_now, skip = bring_both((state, skip_weight), messages[0])
        branch, next_state = vmem_call(
            functools.partial(state_kernel, size, layer, D),
            [((steps, inner), bf16), ((groups, LANES), f32)],
            *arrived, live, real, imag, coupled,
            readout.reshape(chunks, LANES, LANES), skip, state_now,
        )
        states.append(next_state)
        with jax.named_scope(f"c{layer}"):
            branches = [branch] + swaps(branch, "dp", size)
        if layer < LAYERS - 1:
            (part,) = vmem_call(
                functools.partial(output_kernel, size),
                [((count, features), bf16)],
                *branches, out_now,
            )
            with jax.named_scope(f"d{layer}"):
                pieces = [part] + swaps(part, "tp", size)
                *weights, real, imag, coupled = prepare(layer + 1, *raw, after=[part])
            continue
        parts = vmem_call(
            functools.partial(last_output_kernel, size),
            [((steps, features), f32)] + [((steps, features), bf16)] * (size - 1),
            *branches, out_now, rows,
        )
        with jax.named_scope(f"d{layer}"):
            arrived = swaps(parts, "tp", size)
        (mixed,) = vmem_call(final_kernel, [((1, steps, features), bf16)], parts[0], *arrived)
    return mixed, jnp.stack(states)[:, None]


def body(*arguments):
    tokens, lengths, input_map, state = (arguments[i] for i in (0, 1, 8, 12))
    sizes = lax.axis_size("dp"), lax.axis_size("tp")
    if fits(tokens, lengths, state, input_map.shape[2], *sizes):
        return direct_body(*arguments)
    return general_body(*arguments)


def solution(mesh):
    return jax.shard_map(
        body,
        mesh=mesh,
        in_specs=(
            P(("grp", "tp"), None, "dp"),
            P("grp"),
            P(None, "dp"),
            P(None, "dp", "tp"),
            P(None, "dp", "tp"),
            P(None, "tp", None),
            P(None, "tp", None),
            P(None, "tp"),
            P(None, "tp", None, None),
            P(None, "tp", None, None),
            P(None, "tp"),
            P(None, "tp", "dp"),
            P(None, ("grp", "dp"), "tp", None),
        ),
        out_specs=(P(("grp", "tp"), None, "dp"), P(None, ("grp", "dp"), "tp", None)),
        check_vma=False,
    )
```

```python
import functools

import jax
import jax.numpy as jnp
from jax import lax
from jax.experimental import pallas as pl
from jax.experimental.pallas import tpu as pltpu
from jax.sharding import PartitionSpec as P


D = 4096
S5_IN = 16
LAYERS = 2


epsilon = 1e-06


def advance_state(
    drive_value,
    gate_value,
    carried,
    alive_mask,
    decay_rate,
    frequency,
    log_step,
    input_map,
    readout_map,
    skip_row,
):
    seq_count, new_count, inner_width = drive_value.shape
    group_count = inner_width // S5_IN
    state_half = carried.shape[-1] // 2
    step_size = jnp.exp(log_step)[:, None]
    magnitude = jnp.exp(-decay_rate * step_size)
    turn_angle = frequency * step_size
    decay_real = magnitude * jnp.cos(turn_angle)
    decay_imag = magnitude * jnp.sin(turn_angle)
    denominator = decay_rate * decay_rate + frequency * frequency
    coeff_real = (-(decay_real - 1.0) * decay_rate + decay_imag * frequency) / denominator
    coeff_imag = (-decay_imag * decay_rate - (decay_real - 1.0) * frequency) / denominator
    map_real = input_map[..., :state_half].astype(jnp.float32)
    map_imag = input_map[..., state_half:].astype(jnp.float32)
    coupled = jnp.concatenate(
        [
            coeff_real[:, None, :] * map_real - coeff_imag[:, None, :] * map_imag,
            coeff_real[:, None, :] * map_imag + coeff_imag[:, None, :] * map_real,
        ],
        axis=-1,
    )
    inputs = drive_value.astype(jnp.float32).reshape(seq_count, new_count, group_count, S5_IN)
    pushed = jnp.einsum("stgi,giq->stgq", inputs, coupled, precision=lax.Precision.HIGHEST)
    real_state = carried[..., :state_half]
    imag_state = carried[..., state_half:]
    history = []
    for position in range(new_count):
        keep = alive_mask[:, position][:, None, None] > 0.5
        next_real = (
            decay_real * real_state - decay_imag * imag_state + pushed[:, position, :, :state_half]
        )
        next_imag = (
            decay_real * imag_state + decay_imag * real_state + pushed[:, position, :, state_half:]
        )
        real_state = jnp.where(keep, next_real, real_state)
        imag_state = jnp.where(keep, next_imag, imag_state)
        history.append(jnp.concatenate([real_state, -imag_state], axis=-1))
    stacked = jnp.stack(history, axis=1)
    readout = jnp.einsum(
        "stgq,giq->stgi", stacked, readout_map.astype(jnp.float32), precision=lax.Precision.HIGHEST
    )
    readout = readout.reshape(seq_count, new_count, inner_width)
    response = readout + skip_row.astype(jnp.float32) * inputs.reshape(
        seq_count, new_count, inner_width
    )
    branch = (
        jax.nn.gelu(response) * jax.nn.silu(gate_value.astype(jnp.float32)) * alive_mask[:, :, None]
    )
    return (jnp.concatenate([real_state, imag_state], axis=-1), branch.astype(jnp.bfloat16))


def direct(size):
    return 1 < size <= 8 and size & (size - 1) == 0


def swap(value, axis, distance, size):
    return lax.ppermute(value, axis, [(i, i ^ distance) for i in range(size)])


def gather_rows(block, axis, size):
    if not direct(size):
        return lax.all_gather(block, axis, axis=0, tiled=True)
    index = lax.axis_index(axis)
    slots = jnp.stack([block] + [swap(block, axis, k, size) for k in range(1, size)])
    ordered = [lax.dynamic_index_in_dim(slots, index ^ s, 0, keepdims=False) for s in range(size)]
    return jnp.concatenate(ordered, axis=0)


def exchange_rows(value, axis, size):
    index = lax.axis_index(axis)
    rows = value.shape[0] // size
    blocks = [
        lax.dynamic_slice_in_dim(value, (index ^ k) * rows, rows, 0) for k in range(size)
    ]
    return [blocks[0]] + [swap(blocks[k], axis, k, size) for k in range(1, size)]


def split_three(value):
    pieces = []
    for _ in range(3):
        piece = lax.reduce_precision(value, 8, 7)
        pieces.append(piece.astype(jnp.bfloat16))
        value = value - piece
    return pieces


def scatter_projections(part_drive, part_gate, squares, axis, size):
    index = lax.axis_index(axis)
    width = part_drive.shape[1]
    rows = part_drive.shape[0] // size
    if not direct(size):
        total = lax.psum(squares, axis)
        own = lax.dynamic_slice_in_dim(total, index * rows, rows, 0)
        drive, gate = (
            lax.psum_scatter(
                part.astype(jnp.bfloat16), axis, scatter_dimension=0, tiled=True
            ).astype(jnp.float32)
            for part in (part_drive, part_gate)
        )
        return drive, gate, own
    extra = jnp.stack(split_three(squares), axis=1)
    extra = jnp.pad(extra, ((0, 0), (0, 128 - extra.shape[1])))
    message = jnp.concatenate(
        [part_drive.astype(jnp.bfloat16), part_gate.astype(jnp.bfloat16), extra], axis=1
    )
    total = sum(part.astype(jnp.float32) for part in exchange_rows(message, axis, size))
    own = jnp.sum(total[:, 2 * width :], axis=1)
    return total[:, :width], total[:, width : 2 * width], own


def general_body(
    tokens,
    lengths,
    norm_gain,
    input_weight,
    gate_weight,
    decay_rate,
    frequency,
    log_step,
    input_map,
    readout_map,
    skip_weight,
    out_weight,
    state,
):
    own_seqs = state.shape[1]
    block_seqs, new_count, feature_count = tokens.shape
    all_seqs = lengths.shape[0]
    inner_width = input_weight.shape[2]
    dp_index = lax.axis_index("dp")
    tp_index = lax.axis_index("tp")
    dp_size = lax.axis_size("dp")
    tp_size = lax.axis_size("tp")
    positions = lax.broadcasted_iota(jnp.int32, (all_seqs, new_count), 1)
    alive_all = (positions < lengths[:, None]).astype(jnp.float32)
    alive_own = lax.dynamic_slice_in_dim(alive_all, dp_index * own_seqs, own_seqs, 0)
    own_rows = own_seqs * new_count
    block_count = block_seqs * new_count
    states = []
    gathered = gather_rows(tokens.reshape(block_count, feature_count), "tp", tp_size)
    for layer_index in range(LAYERS):
        flattened = gathered.astype(jnp.float32)
        scaled = (flattened * norm_gain[layer_index][None, :]).astype(jnp.bfloat16)
        partial_squares = jnp.sum(flattened * flattened, axis=1)
        part_drive = jnp.dot(scaled, input_weight[layer_index], preferred_element_type=jnp.float32)
        part_gate = jnp.dot(scaled, gate_weight[layer_index], preferred_element_type=jnp.float32)
        summed_drive, summed_gate, own_squares = scatter_projections(
            part_drive, part_gate, partial_squares, "dp", dp_size
        )
        inverse = lax.rsqrt(own_squares / D + epsilon)[:, None]
        drive_value = (
            (inverse * summed_drive).astype(jnp.bfloat16).reshape(own_seqs, new_count, inner_width)
        )
        gate_value = (
            (inverse * summed_gate).astype(jnp.bfloat16).reshape(own_seqs, new_count, inner_width)
        )
        next_state, branch = advance_state(
            drive_value,
            gate_value,
            state[layer_index],
            alive_own,
            decay_rate[layer_index],
            frequency[layer_index],
            log_step[layer_index],
            input_map[layer_index],
            readout_map[layer_index],
            skip_weight[layer_index],
        )
        states.append(next_state)
        weight_now = out_weight[layer_index]
        projected = jnp.dot(
            gather_rows(branch.reshape(own_rows, inner_width), "dp", dp_size),
            weight_now,
            preferred_element_type=jnp.float32,
        ).astype(jnp.bfloat16)
        last = layer_index == LAYERS - 1
        if direct(tp_size) and not last:
            parts = [projected] + [swap(projected, "tp", k, tp_size) for k in range(1, tp_size)]
            total = sum(part.astype(jnp.float32) for part in parts)
            gathered = (flattened + total).astype(jnp.bfloat16)
            continue
        if direct(tp_size):
            parts = exchange_rows(projected, "tp", tp_size)
            branch_sum = sum(part.astype(jnp.float32) for part in parts)
        else:
            branch_sum = lax.psum_scatter(
                projected, "tp", scatter_dimension=0, tiled=True
            ).astype(jnp.float32)
        own_base = lax.dynamic_slice_in_dim(flattened, tp_index * block_count, block_count, 0)
        own_block = (own_base + branch_sum).astype(jnp.bfloat16)
        if not last:
            gathered = lax.all_gather(own_block, "tp", axis=0, tiled=True)
    own_block = own_block.reshape(tokens.shape)
    return (own_block, jnp.stack(states))


LANES = 128
COST = 40000000000
SUBLANES = 8
VMEM = pl.BlockSpec(memory_space=pltpu.VMEM)
HBM = pl.BlockSpec(memory_space=pltpu.MemorySpace.HBM)


def vmem_call(kernel, outs, *operands, in_specs=None, scratch=(), limit=8 << 20, cost=0):
    outs = [jax.ShapeDtypeStruct(shape, dtype) for shape, dtype in outs]
    in_specs = in_specs or [VMEM] * len(operands)
    operands = [
        pltpu.with_memory_space_constraint(operand, pltpu.MemorySpace.HBM) if spec is HBM else operand
        for spec, operand in zip(in_specs, operands)
    ]
    return pl.pallas_call(
        kernel,
        out_shape=outs,
        in_specs=in_specs,
        out_specs=[VMEM] * len(outs),
        scratch_shapes=list(scratch),
        compiler_params=pltpu.CompilerParams(vmem_limit_bytes=limit),
        cost_estimate=pl.CostEstimate(flops=cost, bytes_accessed=0, transcendentals=0) if cost else None,
    )(*operands)


def twice(value):
    return jnp.concatenate([value, value], axis=-1)


def halves(value):
    high = value.astype(jnp.bfloat16)
    low = (value - high.astype(jnp.float32)).astype(jnp.bfloat16)
    return high, low


def group_mask():
    lane = lax.broadcasted_iota(jnp.int32, (SUBLANES, LANES), 1)
    row = lax.broadcasted_iota(jnp.int32, (SUBLANES, LANES), 0)
    return lane // S5_IN == row


def start_copies(sources, targets, semaphores):
    copies = [
        pltpu.make_async_copy(source, target, semaphores.at[i])
        for i, (source, target) in enumerate(zip(sources, targets))
    ]
    for copy in copies:
        copy.start()
    return copies


def wait_copies(copies):
    for copy in copies:
        copy.wait()


def parameter_step(decay, frequency, log_step, map_ref, real_ref, imag_ref, coupled_ref):
    half, groups = decay.shape
    step = jnp.exp(log_step)
    magnitude = jnp.exp(-decay * step)
    angle = frequency * step
    real = magnitude * jnp.cos(angle)
    imag = magnitude * jnp.sin(angle)
    denominator = decay * decay + frequency * frequency
    coeff_real = (imag * frequency - (real - 1.0) * decay) / denominator
    coeff_imag = (-imag * decay - (real - 1.0) * frequency) / denominator

    def across(first, second):
        return jnp.transpose(jnp.concatenate([first, second], axis=0))

    real_ref[...] = across(real, real)
    imag_ref[...] = across(-imag, imag)
    scale_real = across(coeff_real, coeff_real)
    scale_imag = across(-coeff_imag, coeff_imag)
    for chunk in range(groups // SUBLANES):
        rows = slice(chunk * SUBLANES, (chunk + 1) * SUBLANES)
        values = map_ref[rows].astype(jnp.float32).reshape(LANES, LANES)
        spread = [
            jnp.broadcast_to(s[rows][:, None, :], (SUBLANES, S5_IN, LANES)).reshape(LANES, LANES)
            for s in (scale_real, scale_imag)
        ]
        coupled = spread[0] * values + spread[1] * pltpu.roll(values, half, 1)
        high, low = halves(coupled)
        coupled_ref[chunk, :LANES] = high
        coupled_ref[chunk, LANES:] = low


def parameter_kernel(layer, decay_ref, frequency_ref, log_step_ref, map_ref, *refs):
    parameter_step(
        decay_ref[layer], frequency_ref[layer], log_step_ref[layer : layer + 1],
        map_ref.at[layer], *refs[-3:],
    )


def prepare(layer, decay, frequency, log_step, input_map, after=()):
    _, _, groups = decay.shape
    return vmem_call(
        functools.partial(parameter_kernel, layer),
        [((groups, LANES), jnp.float32)] * 2
        + [((groups // SUBLANES, 2 * LANES, LANES), jnp.bfloat16)],
        decay, frequency, log_step, input_map, *after,
        cost=COST,
    )


def small_kernel(steps, lengths_hbm, *refs):
    count = (len(refs) - 3) // 2
    sources, targets = refs[:count], refs[count : 2 * count]
    live_ref, lengths, semaphores = refs[2 * count :]
    copies = start_copies(
        [lengths_hbm, *sources], [lengths, *targets], semaphores
    )
    copies[0].wait()
    length = lengths[lax.axis_index("dp")]
    place = lax.broadcasted_iota(jnp.int32, (steps * SUBLANES, LANES), 0) // SUBLANES
    live_ref[...] = (place < length).astype(jnp.float32)
    wait_copies(copies[1:])


def bring_small(steps, lengths, *arrays):
    return vmem_call(
        functools.partial(small_kernel, steps),
        [(a.shape, a.dtype) for a in arrays] + [((steps * SUBLANES, LANES), jnp.float32)],
        lengths, *arrays,
        in_specs=[HBM] * (1 + len(arrays)),
        scratch=[
            pltpu.SMEM(lengths.shape, jnp.int32),
            pltpu.SemaphoreType.DMA((1 + len(arrays),)),
        ],
        cost=COST,
    )


def swaps(values, axis, size):
    received = {}
    for k in reversed(range(1, size)):
        value = values[k] if isinstance(values, (list, tuple)) else values
        received[k] = swap(value, axis, k, size)
    return [received[k] for k in range(1, size)]


def project(layer, rows, gain_ref, drive_weight_ref, gate_weight_ref, message_refs):
    count = rows.shape[0] // len(message_refs)
    width = drive_weight_ref.shape[2]
    scaled = (rows * gain_ref[layer : layer + 1]).astype(jnp.bfloat16)
    squares = jnp.sum(rows * rows, axis=1, keepdims=True)
    lane = lax.broadcasted_iota(jnp.int32, (rows.shape[0], LANES), 1)
    extra = jnp.zeros((rows.shape[0], LANES), jnp.float32)
    for place in range(3):
        piece = squares.astype(jnp.bfloat16).astype(jnp.float32)
        extra = jnp.where(lane == place, piece, extra)
        squares = squares - piece
    step = min(width, 512)
    parts = [(2 * width, LANES, extra)]
    for base, weight_ref in ((0, drive_weight_ref), (width, gate_weight_ref)):
        for at in range(0, width, step):
            value = jnp.dot(
                scaled, weight_ref[layer, :, at : at + step], preferred_element_type=jnp.float32
            )
            parts.append((base + at, step, value))
    for at, size, value in parts:
        for k, message_ref in enumerate(message_refs):
            block = value[k * count : (k + 1) * count]
            message_ref[:, at : at + size] = block.astype(jnp.bfloat16)


def pick(blocks, offset):
    bit = 1
    while bit < len(blocks):
        on = (offset & bit) != 0
        blocks = [jnp.where(on, blocks[k ^ bit], blocks[k]) for k in range(len(blocks))]
        bit *= 2
    return blocks


def own_offset():
    return lax.axis_index("dp") ^ lax.axis_index("tp")


def first_kernel(size, *refs):
    block_refs, (gain_ref, drive_ref, gate_ref) = refs[:size], refs[size : size + 3]
    message_refs, rows_ref = refs[size + 3 : -1], refs[-1]
    blocks = [ref[...].astype(jnp.float32).reshape(ref.shape[-2:]) for ref in block_refs]
    rows = jnp.concatenate(pick(blocks, own_offset()), axis=0)
    rows_ref[...] = rows
    project(0, rows, gain_ref, drive_ref, gate_ref, message_refs)


def next_kernel(size, layer, base_ref, *refs):
    part_refs, (gain_ref, drive_ref, gate_ref) = refs[:size], refs[size : size + 3]
    message_refs, rows_ref = refs[size + 3 : -1], refs[-1]
    rows = base_ref[...]
    rows = rows + sum(ref[...].astype(jnp.float32) for ref in part_refs)
    rows = rows.astype(jnp.bfloat16).astype(jnp.float32)
    rows_ref[...] = rows
    project(layer, rows, gain_ref, drive_ref, gate_ref, message_refs)


def state_kernel(size, layer, features, *refs):
    message_refs = refs[:size]
    live_ref, real_ref, imag_ref, coupled_ref, readout_ref, skip_ref, state_ref = refs[size:-2]
    branch_ref, next_ref = refs[-2:]
    steps = message_refs[0].shape[0]
    width = branch_ref.shape[1]
    half = LANES // 2
    total = sum(ref[...].astype(jnp.float32) for ref in message_refs)
    squares = jnp.sum(total[:, 2 * width :], axis=1, keepdims=True)
    inverse = lax.rsqrt(squares / features + epsilon)
    drive = (inverse * total[:, :width]).astype(jnp.bfloat16).astype(jnp.float32)
    gate = (inverse * total[:, width : 2 * width]).astype(jnp.bfloat16).astype(jnp.float32)
    live = live_ref[...]
    lane = lax.broadcasted_iota(jnp.int32, (SUBLANES, LANES), 1)
    row = lax.broadcasted_iota(jnp.int32, (SUBLANES, LANES), 0)
    own_group = group_mask()
    keeps = [live[t * SUBLANES : (t + 1) * SUBLANES] > 0.5 for t in range(steps)]
    live_rows = jnp.concatenate(
        [live[t * SUBLANES : t * SUBLANES + 1] for t in range(steps)], axis=0
    )
    sign = jnp.where(lane < half, 1.0, -1.0)
    for chunk in range(width // LANES):
        at = slice(chunk * LANES, (chunk + 1) * LANES)
        groups = slice(chunk * SUBLANES, (chunk + 1) * SUBLANES)
        fed = jnp.concatenate(
            [
                jnp.where(own_group, jnp.broadcast_to(drive[t : t + 1, at], (SUBLANES, LANES)), 0.0)
                for t in range(steps)
            ],
            axis=0,
        ).astype(jnp.bfloat16)
        pushed = jnp.dot(twice(fed), coupled_ref[chunk], preferred_element_type=jnp.float32)
        turned = pltpu.roll(pushed, half, 1)
        real, imag = real_ref[groups], imag_ref[groups]
        value = state_ref[layer, 0, groups]
        other = pltpu.roll(value, half, 1)
        history = []
        for t in range(steps):
            now = slice(t * SUBLANES, (t + 1) * SUBLANES)
            new_value = real * value + imag * other + pushed[now]
            new_other = real * other - imag * value + turned[now]
            value = jnp.where(keeps[t], new_value, value)
            other = jnp.where(keeps[t], new_other, other)
            history.append(value * sign)
        next_ref[groups] = value
        high, low = halves(jnp.concatenate(history, axis=0))
        seen = lax.dot_general(
            jnp.concatenate([high, low], axis=0),
            readout_ref[layer, chunk],
            (((1,), (1,)), ((), ())),
            preferred_element_type=jnp.float32,
        )
        count = steps * SUBLANES
        seen = seen[:count] + seen[count:]
        read = jnp.concatenate(
            [
                jnp.sum(
                    jnp.where(own_group, seen[t * SUBLANES : (t + 1) * SUBLANES], 0.0),
                    axis=0,
                    keepdims=True,
                )
                for t in range(steps)
            ],
            axis=0,
        )
        response = read + skip_ref[layer : layer + 1, at].astype(jnp.float32) * drive[:, at]
        value = jax.nn.gelu(response) * jax.nn.silu(gate[:, at]) * live_rows
        branch_ref[:, at] = value.astype(jnp.bfloat16)


def output_kernel(size, layer, *refs):
    branch_refs, weight_ref, out_ref = refs[:size], refs[size], refs[size + 1]
    rows = jnp.concatenate([ref[...].astype(jnp.float32) for ref in branch_refs], axis=0)
    out_ref[...] = jnp.dot(
        rows.astype(jnp.bfloat16), weight_ref[layer], preferred_element_type=jnp.float32
    ).astype(jnp.bfloat16)


def last_output_kernel(size, layer, *refs):
    branch_refs, weight_ref, base_ref = refs[:size], refs[size], refs[size + 1]
    out_refs = refs[size + 2 :]
    rows = jnp.concatenate([ref[...].astype(jnp.float32) for ref in branch_refs], axis=0)
    value = jnp.dot(rows.astype(jnp.bfloat16), weight_ref[layer], preferred_element_type=jnp.float32)
    count = rows.shape[0] // size
    blocks = [value[k * count : (k + 1) * count] for k in range(size)]
    offset = own_offset()
    blocks = pick(blocks, offset)
    base = base_ref[...]
    bases = pick([base[k * count : (k + 1) * count] for k in range(size)], offset)
    out_refs[0][...] = bases[0] + blocks[0]
    for out_ref, block in zip(out_refs[1:], blocks[1:]):
        out_ref[...] = block.astype(jnp.bfloat16)


def final_kernel(own_ref, *refs):
    total = own_ref[...] + sum(ref[...].astype(jnp.float32) for ref in refs[:-1])
    refs[-1][0] = total.astype(jnp.bfloat16)


def fits(tokens, lengths, state, map_rows, dp_size, tp_size):
    whole_groups = state.shape[2] % LANES == 0 and state.shape[3] == LANES
    one_each = tokens.shape[0] == 1 and state.shape[1] == 1
    equal = dp_size == tp_size == lengths.shape[0]
    return direct(dp_size) and equal and one_each and whole_groups and map_rows == S5_IN


def direct_steps(
    tokens,
    lengths,
    norm_gain,
    input_weight,
    gate_weight,
    decay_rate,
    frequency,
    log_step,
    input_map,
    readout_map,
    skip_weight,
    out_weight,
    state,
):
    size = lax.axis_size("dp")
    _, steps, features = tokens.shape
    inner = input_weight.shape[2]
    groups = state.shape[2]
    chunks = groups // SUBLANES
    count = size * steps
    bf16, f32 = jnp.bfloat16, jnp.float32
    message = [((steps, 2 * inner + LANES), bf16)] * size
    rows_shape = ((count, features), f32)
    readout = readout_map.reshape(LAYERS, chunks, LANES, LANES)
    projections = (input_weight, gate_weight)
    decay, frequency = (jnp.swapaxes(value, 1, 2) for value in (decay_rate, frequency))
    raw = (decay, frequency, log_step, input_map)
    own = tokens.reshape(steps, features)
    own, gain, live = bring_small(steps, lengths, own, norm_gain)
    pieces = swaps(own, "tp", size)
    pieces = [own] + pieces
    real, imag, coupled = prepare(0, *raw)
    weights = projections
    states = []
    for layer in range(LAYERS):
        if layer == 0:
            kernel, base = functools.partial(first_kernel, size), []
        else:
            kernel, base = functools.partial(next_kernel, size, layer), [rows]
        results = vmem_call(kernel, message + [rows_shape], *base, *pieces, gain, *weights)
        messages, rows = results[:size], results[size]
        arrived = [messages[0]] + swaps(messages, "dp", size)
        out_now = out_weight
        branch, next_state = vmem_call(
            functools.partial(state_kernel, size, layer, D),
            [((steps, inner), bf16), ((groups, LANES), f32)],
            *arrived, live, real, imag, coupled,
            readout, skip_weight, state,
        )
        states.append(next_state)
        branches = [branch] + swaps(branch, "dp", size)
        if layer < LAYERS - 1:
            (part,) = vmem_call(
                functools.partial(output_kernel, size, layer),
                [((count, features), bf16)],
                *branches, out_now,
            )
            pieces = [part] + swaps(part, "tp", size)
            real, imag, coupled = prepare(layer + 1, *raw, after=[part])
            continue
        parts = vmem_call(
            functools.partial(last_output_kernel, size, layer),
            [((steps, features), f32)] + [((steps, features), bf16)] * (size - 1),
            *branches, out_now, rows,
        )
        arrived = swaps(parts, "tp", size)
        (mixed,) = vmem_call(final_kernel, [((1, steps, features), bf16)], parts[0], *arrived)
    return mixed, jnp.stack(states)[:, None]


def body(*arguments):
    tokens, lengths, input_map, state = (arguments[i] for i in (0, 1, 8, 12))
    sizes = lax.axis_size("dp"), lax.axis_size("tp")
    if fits(tokens, lengths, state, input_map.shape[2], *sizes):
        return direct_steps(*arguments)
    return general_body(*arguments)


def solution(mesh):
    step = jax.shard_map(
        body,
        mesh=mesh,
        in_specs=(
            P(("grp", "tp"), None, "dp"),
            P("grp"),
            P(None, "dp"),
            P(None, "dp", "tp"),
            P(None, "dp", "tp"),
            P(None, "tp", None),
            P(None, "tp", None),
            P(None, "tp"),
            P(None, "tp", None, None),
            P(None, "tp", None, None),
            P(None, "tp"),
            P(None, "tp", "dp"),
            P(None, ("grp", "dp"), "tp", None),
        ),
        out_specs=(P(("grp", "tp"), None, "dp"), P(None, ("grp", "dp"), "tp", None)),
        check_vma=False,
    )
    size = mesh.shape["dp"]
    if size != mesh.shape["tp"] or not direct(size):
        return step
    return step
```

```python
import functools

import jax
import jax.numpy as jnp
from jax import lax
from jax.experimental import pallas as pl
from jax.experimental.pallas import tpu as pltpu
from jax.sharding import PartitionSpec as P


D = 4096
S5_IN = 16
LAYERS = 2


epsilon = 1e-06


def advance_state(
    drive_value,
    gate_value,
    carried,
    alive_mask,
    decay_rate,
    frequency,
    log_step,
    input_map,
    readout_map,
    skip_row,
):
    seq_count, new_count, inner_width = drive_value.shape
    group_count = inner_width // S5_IN
    state_half = carried.shape[-1] // 2
    step_size = jnp.exp(log_step)[:, None]
    magnitude = jnp.exp(-decay_rate * step_size)
    turn_angle = frequency * step_size
    decay_real = magnitude * jnp.cos(turn_angle)
    decay_imag = magnitude * jnp.sin(turn_angle)
    denominator = decay_rate * decay_rate + frequency * frequency
    coeff_real = (-(decay_real - 1.0) * decay_rate + decay_imag * frequency) / denominator
    coeff_imag = (-decay_imag * decay_rate - (decay_real - 1.0) * frequency) / denominator
    map_real = input_map[..., :state_half].astype(jnp.float32)
    map_imag = input_map[..., state_half:].astype(jnp.float32)
    coupled = jnp.concatenate(
        [
            coeff_real[:, None, :] * map_real - coeff_imag[:, None, :] * map_imag,
            coeff_real[:, None, :] * map_imag + coeff_imag[:, None, :] * map_real,
        ],
        axis=-1,
    )
    inputs = drive_value.astype(jnp.float32).reshape(seq_count, new_count, group_count, S5_IN)
    pushed = jnp.einsum("stgi,giq->stgq", inputs, coupled, precision=lax.Precision.HIGHEST)
    real_state = carried[..., :state_half]
    imag_state = carried[..., state_half:]
    history = []
    for position in range(new_count):
        keep = alive_mask[:, position][:, None, None] > 0.5
        next_real = (
            decay_real * real_state - decay_imag * imag_state + pushed[:, position, :, :state_half]
        )
        next_imag = (
            decay_real * imag_state + decay_imag * real_state + pushed[:, position, :, state_half:]
        )
        real_state = jnp.where(keep, next_real, real_state)
        imag_state = jnp.where(keep, next_imag, imag_state)
        history.append(jnp.concatenate([real_state, -imag_state], axis=-1))
    stacked = jnp.stack(history, axis=1)
    readout = jnp.einsum(
        "stgq,giq->stgi", stacked, readout_map.astype(jnp.float32), precision=lax.Precision.HIGHEST
    )
    readout = readout.reshape(seq_count, new_count, inner_width)
    response = readout + skip_row.astype(jnp.float32) * inputs.reshape(
        seq_count, new_count, inner_width
    )
    branch = (
        jax.nn.gelu(response) * jax.nn.silu(gate_value.astype(jnp.float32)) * alive_mask[:, :, None]
    )
    return (jnp.concatenate([real_state, imag_state], axis=-1), branch.astype(jnp.bfloat16))


def direct(size):
    return 1 < size <= 8 and size & (size - 1) == 0


def swap(value, axis, distance, size):
    return lax.ppermute(value, axis, [(i, i ^ distance) for i in range(size)])


def gather_rows(block, axis, size):
    if not direct(size):
        return lax.all_gather(block, axis, axis=0, tiled=True)
    index = lax.axis_index(axis)
    slots = jnp.stack([block] + [swap(block, axis, k, size) for k in range(1, size)])
    ordered = [lax.dynamic_index_in_dim(slots, index ^ s, 0, keepdims=False) for s in range(size)]
    return jnp.concatenate(ordered, axis=0)


def exchange_rows(value, axis, size):
    index = lax.axis_index(axis)
    rows = value.shape[0] // size
    blocks = [
        lax.dynamic_slice_in_dim(value, (index ^ k) * rows, rows, 0) for k in range(size)
    ]
    return [blocks[0]] + [swap(blocks[k], axis, k, size) for k in range(1, size)]


def split_three(value):
    pieces = []
    for _ in range(3):
        piece = lax.reduce_precision(value, 8, 7)
        pieces.append(piece.astype(jnp.bfloat16))
        value = value - piece
    return pieces


def scatter_projections(part_drive, part_gate, squares, axis, size):
    index = lax.axis_index(axis)
    width = part_drive.shape[1]
    rows = part_drive.shape[0] // size
    if not direct(size):
        total = lax.psum(squares, axis)
        own = lax.dynamic_slice_in_dim(total, index * rows, rows, 0)
        drive, gate = (
            lax.psum_scatter(
                part.astype(jnp.bfloat16), axis, scatter_dimension=0, tiled=True
            ).astype(jnp.float32)
            for part in (part_drive, part_gate)
        )
        return drive, gate, own
    extra = jnp.stack(split_three(squares), axis=1)
    extra = jnp.pad(extra, ((0, 0), (0, 128 - extra.shape[1])))
    message = jnp.concatenate(
        [part_drive.astype(jnp.bfloat16), part_gate.astype(jnp.bfloat16), extra], axis=1
    )
    total = sum(part.astype(jnp.float32) for part in exchange_rows(message, axis, size))
    own = jnp.sum(total[:, 2 * width :], axis=1)
    return total[:, :width], total[:, width : 2 * width], own


def general_body(
    tokens,
    lengths,
    norm_gain,
    input_weight,
    gate_weight,
    decay_rate,
    frequency,
    log_step,
    input_map,
    readout_map,
    skip_weight,
    out_weight,
    state,
):
    own_seqs = state.shape[1]
    block_seqs, new_count, feature_count = tokens.shape
    all_seqs = lengths.shape[0]
    inner_width = input_weight.shape[2]
    dp_index = lax.axis_index("dp")
    tp_index = lax.axis_index("tp")
    dp_size = lax.axis_size("dp")
    tp_size = lax.axis_size("tp")
    positions = lax.broadcasted_iota(jnp.int32, (all_seqs, new_count), 1)
    alive_all = (positions < lengths[:, None]).astype(jnp.float32)
    alive_own = lax.dynamic_slice_in_dim(alive_all, dp_index * own_seqs, own_seqs, 0)
    own_rows = own_seqs * new_count
    block_count = block_seqs * new_count
    states = []
    gathered = gather_rows(tokens.reshape(block_count, feature_count), "tp", tp_size)
    for layer_index in range(LAYERS):
        flattened = gathered.astype(jnp.float32)
        scaled = (flattened * norm_gain[layer_index][None, :]).astype(jnp.bfloat16)
        partial_squares = jnp.sum(flattened * flattened, axis=1)
        part_drive = jnp.dot(scaled, input_weight[layer_index], preferred_element_type=jnp.float32)
        part_gate = jnp.dot(scaled, gate_weight[layer_index], preferred_element_type=jnp.float32)
        summed_drive, summed_gate, own_squares = scatter_projections(
            part_drive, part_gate, partial_squares, "dp", dp_size
        )
        inverse = lax.rsqrt(own_squares / D + epsilon)[:, None]
        drive_value = (
            (inverse * summed_drive).astype(jnp.bfloat16).reshape(own_seqs, new_count, inner_width)
        )
        gate_value = (
            (inverse * summed_gate).astype(jnp.bfloat16).reshape(own_seqs, new_count, inner_width)
        )
        next_state, branch = advance_state(
            drive_value,
            gate_value,
            state[layer_index],
            alive_own,
            decay_rate[layer_index],
            frequency[layer_index],
            log_step[layer_index],
            input_map[layer_index],
            readout_map[layer_index],
            skip_weight[layer_index],
        )
        states.append(next_state)
        weight_now = out_weight[layer_index]
        projected = jnp.dot(
            gather_rows(branch.reshape(own_rows, inner_width), "dp", dp_size),
            weight_now,
            preferred_element_type=jnp.float32,
        ).astype(jnp.bfloat16)
        last = layer_index == LAYERS - 1
        if direct(tp_size) and not last:
            parts = [projected] + [swap(projected, "tp", k, tp_size) for k in range(1, tp_size)]
            total = sum(part.astype(jnp.float32) for part in parts)
            gathered = (flattened + total).astype(jnp.bfloat16)
            continue
        if direct(tp_size):
            parts = exchange_rows(projected, "tp", tp_size)
            branch_sum = sum(part.astype(jnp.float32) for part in parts)
        else:
            branch_sum = lax.psum_scatter(
                projected, "tp", scatter_dimension=0, tiled=True
            ).astype(jnp.float32)
        own_base = lax.dynamic_slice_in_dim(flattened, tp_index * block_count, block_count, 0)
        own_block = (own_base + branch_sum).astype(jnp.bfloat16)
        if not last:
            gathered = lax.all_gather(own_block, "tp", axis=0, tiled=True)
    own_block = own_block.reshape(tokens.shape)
    return (own_block, jnp.stack(states))


LANES = 128
COST = 40000000000
SUBLANES = 8
VMEM = pl.BlockSpec(memory_space=pltpu.VMEM)
HBM = pl.BlockSpec(memory_space=pltpu.MemorySpace.HBM)


def vmem_call(kernel, outs, *operands, in_specs=None, scratch=(), limit=8 << 20, cost=0):
    outs = [jax.ShapeDtypeStruct(shape, dtype) for shape, dtype in outs]
    in_specs = in_specs or [VMEM] * len(operands)
    operands = [
        pltpu.with_memory_space_constraint(operand, pltpu.MemorySpace.HBM) if spec is HBM else operand
        for spec, operand in zip(in_specs, operands)
    ]
    return pl.pallas_call(
        kernel,
        out_shape=outs,
        in_specs=in_specs,
        out_specs=[VMEM] * len(outs),
        scratch_shapes=list(scratch),
        compiler_params=pltpu.CompilerParams(vmem_limit_bytes=limit),
        cost_estimate=pl.CostEstimate(flops=cost, bytes_accessed=0, transcendentals=0) if cost else None,
    )(*operands)


def twice(value):
    return jnp.concatenate([value, value], axis=-1)


def halves(value):
    high = value.astype(jnp.bfloat16)
    low = (value - high.astype(jnp.float32)).astype(jnp.bfloat16)
    return high, low


def group_mask():
    lane = lax.broadcasted_iota(jnp.int32, (SUBLANES, LANES), 1)
    row = lax.broadcasted_iota(jnp.int32, (SUBLANES, LANES), 0)
    return lane // S5_IN == row


def start_copies(sources, targets, semaphores):
    copies = [
        pltpu.make_async_copy(source, target, semaphores.at[i])
        for i, (source, target) in enumerate(zip(sources, targets))
    ]
    for copy in copies:
        copy.start()
    return copies


def wait_copies(copies):
    for copy in copies:
        copy.wait()


def parameter_step(
    decay, frequency, log_step, map_ref, readout_ref, real_ref, imag_ref, coupled_ref, seen_ref
):
    half, groups = decay.shape
    step = jnp.exp(log_step)
    magnitude = jnp.exp(-decay * step)
    angle = frequency * step
    real = magnitude * jnp.cos(angle)
    imag = magnitude * jnp.sin(angle)
    denominator = decay * decay + frequency * frequency
    coeff_real = (imag * frequency - (real - 1.0) * decay) / denominator
    coeff_imag = (-imag * decay - (real - 1.0) * frequency) / denominator

    def across(first, second):
        return jnp.transpose(jnp.concatenate([first, second], axis=0))

    real_ref[...] = across(real, real)
    imag_ref[...] = across(-imag, imag)
    scale_real = across(coeff_real, coeff_real)
    scale_imag = across(-coeff_imag, coeff_imag)
    upper = lax.broadcasted_iota(jnp.int32, (LANES, LANES), 0) < half
    for chunk in range(groups // SUBLANES):
        rows = slice(chunk * SUBLANES, (chunk + 1) * SUBLANES)
        values = map_ref[rows].astype(jnp.float32).reshape(LANES, LANES)
        spread = [
            jnp.broadcast_to(s[rows][:, None, :], (SUBLANES, S5_IN, LANES)).reshape(LANES, LANES)
            for s in (scale_real, scale_imag)
        ]
        coupled = spread[0] * values + spread[1] * pltpu.roll(values, half, 1)
        high, low = halves(coupled)
        coupled_ref[chunk, :LANES] = high
        coupled_ref[chunk, LANES:] = low
        seen = jnp.transpose(readout_ref[rows].astype(jnp.float32).reshape(LANES, LANES))
        seen_ref[chunk] = jnp.where(upper, seen, -seen).astype(jnp.bfloat16)


def parameter_kernel(
    layer, decay_ref, frequency_ref, log_step_ref, map_ref, readout_ref, *refs
):
    parameter_step(
        decay_ref[layer], frequency_ref[layer], log_step_ref[layer : layer + 1],
        map_ref.at[layer], readout_ref.at[layer], *refs[-4:],
    )


def prepare(layer, decay, frequency, log_step, input_map, readout_map, after=()):
    _, _, groups = decay.shape
    return vmem_call(
        functools.partial(parameter_kernel, layer),
        [((groups, LANES), jnp.float32)] * 2
        + [((groups // SUBLANES, rows, LANES), jnp.bfloat16) for rows in (2 * LANES, LANES)],
        decay, frequency, log_step, input_map, readout_map, *after,
        cost=COST,
    )


def small_kernel(steps, lengths_hbm, *refs):
    count = (len(refs) - 3) // 2
    sources, targets = refs[:count], refs[count : 2 * count]
    live_ref, lengths, semaphores = refs[2 * count :]
    copies = start_copies(
        [lengths_hbm, *sources], [lengths, *targets], semaphores
    )
    copies[0].wait()
    length = lengths[lax.axis_index("dp")]
    place = lax.broadcasted_iota(jnp.int32, (steps * SUBLANES, LANES), 0) // SUBLANES
    live_ref[...] = (place < length).astype(jnp.float32)
    wait_copies(copies[1:])


def bring_small(steps, lengths, *arrays):
    return vmem_call(
        functools.partial(small_kernel, steps),
        [(a.shape, a.dtype) for a in arrays] + [((steps * SUBLANES, LANES), jnp.float32)],
        lengths, *arrays,
        in_specs=[HBM] * (1 + len(arrays)),
        scratch=[
            pltpu.SMEM(lengths.shape, jnp.int32),
            pltpu.SemaphoreType.DMA((1 + len(arrays),)),
        ],
        cost=COST,
    )


def swaps(values, axis, size):
    received = {}
    for k in reversed(range(1, size)):
        value = values[k] if isinstance(values, (list, tuple)) else values
        received[k] = swap(value, axis, k, size)
    return [received[k] for k in range(1, size)]


def project(layer, rows, gain_ref, drive_weight_ref, gate_weight_ref, message_refs):
    count = rows.shape[0] // len(message_refs)
    width = drive_weight_ref.shape[2]
    scaled = (rows * gain_ref[layer : layer + 1]).astype(jnp.bfloat16)
    squares = jnp.sum(rows * rows, axis=1, keepdims=True)
    lane = lax.broadcasted_iota(jnp.int32, (rows.shape[0], LANES), 1)
    extra = jnp.zeros((rows.shape[0], LANES), jnp.float32)
    for place in range(3):
        piece = squares.astype(jnp.bfloat16).astype(jnp.float32)
        extra = jnp.where(lane == place, piece, extra)
        squares = squares - piece
    step = min(width, 512)
    parts = [(2 * width, LANES, extra)]
    for base, weight_ref in ((0, drive_weight_ref), (width, gate_weight_ref)):
        for at in range(0, width, step):
            value = jnp.dot(
                scaled, weight_ref[layer, :, at : at + step], preferred_element_type=jnp.float32
            )
            parts.append((base + at, step, value))
    for at, size, value in parts:
        for k, message_ref in enumerate(message_refs):
            block = value[k * count : (k + 1) * count]
            message_ref[:, at : at + size] = block.astype(jnp.bfloat16)


def pick(blocks, offset):
    bit = 1
    while bit < len(blocks):
        on = (offset & bit) != 0
        blocks = [jnp.where(on, blocks[k ^ bit], blocks[k]) for k in range(len(blocks))]
        bit *= 2
    return blocks


def own_offset():
    return lax.axis_index("dp") ^ lax.axis_index("tp")


def first_kernel(size, *refs):
    block_refs, (gain_ref, drive_ref, gate_ref) = refs[:size], refs[size : size + 3]
    message_refs, rows_ref = refs[size + 3 : -1], refs[-1]
    blocks = [ref[...].astype(jnp.float32).reshape(ref.shape[-2:]) for ref in block_refs]
    rows = jnp.concatenate(pick(blocks, own_offset()), axis=0)
    rows_ref[...] = rows
    project(0, rows, gain_ref, drive_ref, gate_ref, message_refs)


def next_kernel(size, layer, base_ref, *refs):
    part_refs, (gain_ref, drive_ref, gate_ref) = refs[:size], refs[size : size + 3]
    message_refs, rows_ref = refs[size + 3 : -1], refs[-1]
    rows = base_ref[...]
    rows = rows + sum(ref[...].astype(jnp.float32) for ref in part_refs)
    rows = rows.astype(jnp.bfloat16).astype(jnp.float32)
    rows_ref[...] = rows
    project(layer, rows, gain_ref, drive_ref, gate_ref, message_refs)


def state_kernel(size, layer, features, *refs):
    message_refs = refs[:size]
    live_ref, real_ref, imag_ref, coupled_ref, seen_ref, skip_ref, state_ref = refs[size:-2]
    branch_ref, next_ref = refs[-2:]
    steps = message_refs[0].shape[0]
    width = branch_ref.shape[1]
    half = LANES // 2
    total = sum(ref[...].astype(jnp.float32) for ref in message_refs)
    squares = jnp.sum(total[:, 2 * width :], axis=1, keepdims=True)
    inverse = lax.rsqrt(squares / features + epsilon)
    drive = (inverse * total[:, :width]).astype(jnp.bfloat16).astype(jnp.float32)
    gate = (inverse * total[:, width : 2 * width]).astype(jnp.bfloat16).astype(jnp.float32)
    live = live_ref[...]
    own_group = group_mask()
    keeps = [live[t * SUBLANES : (t + 1) * SUBLANES] > 0.5 for t in range(steps)]
    live_rows = jnp.concatenate(
        [live[t * SUBLANES : t * SUBLANES + 1] for t in range(steps)], axis=0
    )
    for chunk in range(width // LANES):
        at = slice(chunk * LANES, (chunk + 1) * LANES)
        groups = slice(chunk * SUBLANES, (chunk + 1) * SUBLANES)
        fed = jnp.concatenate(
            [
                jnp.where(own_group, jnp.broadcast_to(drive[t : t + 1, at], (SUBLANES, LANES)), 0.0)
                for t in range(steps)
            ],
            axis=0,
        ).astype(jnp.bfloat16)
        pushed = jnp.dot(twice(fed), coupled_ref[chunk], preferred_element_type=jnp.float32)
        turned = pltpu.roll(pushed, half, 1)
        real, imag = real_ref[groups], imag_ref[groups]
        value = state_ref[layer, 0, groups]
        other = pltpu.roll(value, half, 1)
        history = []
        for t in range(steps):
            now = slice(t * SUBLANES, (t + 1) * SUBLANES)
            new_value = real * value + imag * other + pushed[now]
            new_other = real * other - imag * value + turned[now]
            value = jnp.where(keeps[t], new_value, value)
            other = jnp.where(keeps[t], new_other, other)
            history.append(value)
        next_ref[groups] = value
        high, low = halves(jnp.concatenate(history, axis=0))
        seen = jnp.dot(
            jnp.concatenate([high, low], axis=0), seen_ref[chunk], preferred_element_type=jnp.float32
        )
        count = steps * SUBLANES
        seen = seen[:count] + seen[count:]
        read = jnp.concatenate(
            [
                jnp.sum(
                    jnp.where(own_group, seen[t * SUBLANES : (t + 1) * SUBLANES], 0.0),
                    axis=0,
                    keepdims=True,
                )
                for t in range(steps)
            ],
            axis=0,
        )
        response = read + skip_ref[layer : layer + 1, at].astype(jnp.float32) * drive[:, at]
        value = jax.nn.gelu(response) * jax.nn.silu(gate[:, at]) * live_rows
        branch_ref[:, at] = value.astype(jnp.bfloat16)


def output_kernel(size, layer, *refs):
    branch_refs, weight_ref, out_ref = refs[:size], refs[size], refs[size + 1]
    rows = jnp.concatenate([ref[...].astype(jnp.float32) for ref in branch_refs], axis=0)
    out_ref[...] = jnp.dot(
        rows.astype(jnp.bfloat16), weight_ref[layer], preferred_element_type=jnp.float32
    ).astype(jnp.bfloat16)


def last_output_kernel(size, layer, *refs):
    branch_refs, weight_ref, base_ref = refs[:size], refs[size], refs[size + 1]
    out_refs = refs[size + 2 :]
    rows = jnp.concatenate([ref[...].astype(jnp.float32) for ref in branch_refs], axis=0)
    value = jnp.dot(rows.astype(jnp.bfloat16), weight_ref[layer], preferred_element_type=jnp.float32)
    count = rows.shape[0] // size
    blocks = [value[k * count : (k + 1) * count] for k in range(size)]
    offset = own_offset()
    blocks = pick(blocks, offset)
    base = base_ref[...]
    bases = pick([base[k * count : (k + 1) * count] for k in range(size)], offset)
    out_refs[0][...] = bases[0] + blocks[0]
    for out_ref, block in zip(out_refs[1:], blocks[1:]):
        out_ref[...] = block.astype(jnp.bfloat16)


def final_kernel(own_ref, *refs):
    total = own_ref[...] + sum(ref[...].astype(jnp.float32) for ref in refs[:-1])
    refs[-1][0] = total.astype(jnp.bfloat16)


def fits(tokens, lengths, state, map_rows, dp_size, tp_size):
    whole_groups = state.shape[2] % LANES == 0 and state.shape[3] == LANES
    one_each = tokens.shape[0] == 1 and state.shape[1] == 1
    equal = dp_size == tp_size == lengths.shape[0]
    return direct(dp_size) and equal and one_each and whole_groups and map_rows == S5_IN


def direct_steps(
    tokens,
    lengths,
    norm_gain,
    input_weight,
    gate_weight,
    decay_rate,
    frequency,
    log_step,
    input_map,
    readout_map,
    skip_weight,
    out_weight,
    state,
):
    size = lax.axis_size("dp")
    _, steps, features = tokens.shape
    inner = input_weight.shape[2]
    groups = state.shape[2]
    count = size * steps
    bf16, f32 = jnp.bfloat16, jnp.float32
    message = [((steps, 2 * inner + LANES), bf16)] * size
    rows_shape = ((count, features), f32)
    projections = (input_weight, gate_weight)
    decay, frequency = (jnp.swapaxes(value, 1, 2) for value in (decay_rate, frequency))
    raw = (decay, frequency, log_step, input_map, readout_map)
    own = tokens.reshape(steps, features)
    own, gain, live = bring_small(steps, lengths, own, norm_gain)
    pieces = swaps(own, "tp", size)
    pieces = [own] + pieces
    real, imag, coupled, seen = prepare(0, *raw)
    weights = projections
    states = []
    for layer in range(LAYERS):
        if layer == 0:
            kernel, base = functools.partial(first_kernel, size), []
        else:
            kernel, base = functools.partial(next_kernel, size, layer), [rows]
        results = vmem_call(kernel, message + [rows_shape], *base, *pieces, gain, *weights)
        messages, rows = results[:size], results[size]
        arrived = [messages[0]] + swaps(messages, "dp", size)
        out_now = out_weight
        branch, next_state = vmem_call(
            functools.partial(state_kernel, size, layer, D),
            [((steps, inner), bf16), ((groups, LANES), f32)],
            *arrived, live, real, imag, coupled,
            seen, skip_weight, state,
        )
        states.append(next_state)
        branches = [branch] + swaps(branch, "dp", size)
        if layer < LAYERS - 1:
            (part,) = vmem_call(
                functools.partial(output_kernel, size, layer),
                [((count, features), bf16)],
                *branches, out_now,
            )
            pieces = [part] + swaps(part, "tp", size)
            real, imag, coupled, seen = prepare(layer + 1, *raw, after=[part])
            continue
        parts = vmem_call(
            functools.partial(last_output_kernel, size, layer),
            [((steps, features), f32)] + [((steps, features), bf16)] * (size - 1),
            *branches, out_now, rows,
        )
        arrived = swaps(parts, "tp", size)
        (mixed,) = vmem_call(final_kernel, [((1, steps, features), bf16)], parts[0], *arrived)
    return mixed, jnp.stack(states)[:, None]


def body(*arguments):
    tokens, lengths, input_map, state = (arguments[i] for i in (0, 1, 8, 12))
    sizes = lax.axis_size("dp"), lax.axis_size("tp")
    if fits(tokens, lengths, state, input_map.shape[2], *sizes):
        return direct_steps(*arguments)
    return general_body(*arguments)


def solution(mesh):
    step = jax.shard_map(
        body,
        mesh=mesh,
        in_specs=(
            P(("grp", "tp"), None, "dp"),
            P("grp"),
            P(None, "dp"),
            P(None, "dp", "tp"),
            P(None, "dp", "tp"),
            P(None, "tp", None),
            P(None, "tp", None),
            P(None, "tp"),
            P(None, "tp", None, None),
            P(None, "tp", None, None),
            P(None, "tp"),
            P(None, "tp", "dp"),
            P(None, ("grp", "dp"), "tp", None),
        ),
        out_specs=(P(("grp", "tp"), None, "dp"), P(None, ("grp", "dp"), "tp", None)),
        check_vma=False,
    )
    size = mesh.shape["dp"]
    if size != mesh.shape["tp"] or not direct(size):
        return step
    return step
```

```python
import functools

import jax
import jax.numpy as jnp
from jax import lax
from jax.experimental import pallas as pl
from jax.experimental.pallas import tpu as pltpu
from jax.sharding import PartitionSpec as P


D = 4096
S5_IN = 16
LAYERS = 2


epsilon = 1e-06


def advance_state(
    drive_value,
    gate_value,
    carried,
    alive_mask,
    decay_rate,
    frequency,
    log_step,
    input_map,
    readout_map,
    skip_row,
):
    seq_count, new_count, inner_width = drive_value.shape
    group_count = inner_width // S5_IN
    state_half = carried.shape[-1] // 2
    step_size = jnp.exp(log_step)[:, None]
    magnitude = jnp.exp(-decay_rate * step_size)
    turn_angle = frequency * step_size
    decay_real = magnitude * jnp.cos(turn_angle)
    decay_imag = magnitude * jnp.sin(turn_angle)
    denominator = decay_rate * decay_rate + frequency * frequency
    coeff_real = (-(decay_real - 1.0) * decay_rate + decay_imag * frequency) / denominator
    coeff_imag = (-decay_imag * decay_rate - (decay_real - 1.0) * frequency) / denominator
    map_real = input_map[..., :state_half].astype(jnp.float32)
    map_imag = input_map[..., state_half:].astype(jnp.float32)
    coupled = jnp.concatenate(
        [
            coeff_real[:, None, :] * map_real - coeff_imag[:, None, :] * map_imag,
            coeff_real[:, None, :] * map_imag + coeff_imag[:, None, :] * map_real,
        ],
        axis=-1,
    )
    inputs = drive_value.astype(jnp.float32).reshape(seq_count, new_count, group_count, S5_IN)
    pushed = jnp.einsum("stgi,giq->stgq", inputs, coupled, precision=lax.Precision.HIGHEST)
    real_state = carried[..., :state_half]
    imag_state = carried[..., state_half:]
    history = []
    for position in range(new_count):
        keep = alive_mask[:, position][:, None, None] > 0.5
        next_real = (
            decay_real * real_state - decay_imag * imag_state + pushed[:, position, :, :state_half]
        )
        next_imag = (
            decay_real * imag_state + decay_imag * real_state + pushed[:, position, :, state_half:]
        )
        real_state = jnp.where(keep, next_real, real_state)
        imag_state = jnp.where(keep, next_imag, imag_state)
        history.append(jnp.concatenate([real_state, -imag_state], axis=-1))
    stacked = jnp.stack(history, axis=1)
    readout = jnp.einsum(
        "stgq,giq->stgi", stacked, readout_map.astype(jnp.float32), precision=lax.Precision.HIGHEST
    )
    readout = readout.reshape(seq_count, new_count, inner_width)
    response = readout + skip_row.astype(jnp.float32) * inputs.reshape(
        seq_count, new_count, inner_width
    )
    branch = (
        jax.nn.gelu(response) * jax.nn.silu(gate_value.astype(jnp.float32)) * alive_mask[:, :, None]
    )
    return (jnp.concatenate([real_state, imag_state], axis=-1), branch.astype(jnp.bfloat16))


def direct(size):
    return 1 < size <= 8 and size & (size - 1) == 0


def swap(value, axis, distance, size):
    return lax.ppermute(value, axis, [(i, i ^ distance) for i in range(size)])


def gather_rows(block, axis, size):
    if not direct(size):
        return lax.all_gather(block, axis, axis=0, tiled=True)
    index = lax.axis_index(axis)
    slots = jnp.stack([block] + [swap(block, axis, k, size) for k in range(1, size)])
    ordered = [lax.dynamic_index_in_dim(slots, index ^ s, 0, keepdims=False) for s in range(size)]
    return jnp.concatenate(ordered, axis=0)


def exchange_rows(value, axis, size):
    index = lax.axis_index(axis)
    rows = value.shape[0] // size
    blocks = [
        lax.dynamic_slice_in_dim(value, (index ^ k) * rows, rows, 0) for k in range(size)
    ]
    return [blocks[0]] + [swap(blocks[k], axis, k, size) for k in range(1, size)]


def split_three(value):
    pieces = []
    for _ in range(3):
        piece = lax.reduce_precision(value, 8, 7)
        pieces.append(piece.astype(jnp.bfloat16))
        value = value - piece
    return pieces


def scatter_projections(part_drive, part_gate, squares, axis, size):
    index = lax.axis_index(axis)
    width = part_drive.shape[1]
    rows = part_drive.shape[0] // size
    if not direct(size):
        total = lax.psum(squares, axis)
        own = lax.dynamic_slice_in_dim(total, index * rows, rows, 0)
        drive, gate = (
            lax.psum_scatter(
                part.astype(jnp.bfloat16), axis, scatter_dimension=0, tiled=True
            ).astype(jnp.float32)
            for part in (part_drive, part_gate)
        )
        return drive, gate, own
    extra = jnp.stack(split_three(squares), axis=1)
    extra = jnp.pad(extra, ((0, 0), (0, 128 - extra.shape[1])))
    message = jnp.concatenate(
        [part_drive.astype(jnp.bfloat16), part_gate.astype(jnp.bfloat16), extra], axis=1
    )
    total = sum(part.astype(jnp.float32) for part in exchange_rows(message, axis, size))
    own = jnp.sum(total[:, 2 * width :], axis=1)
    return total[:, :width], total[:, width : 2 * width], own


def general_body(
    tokens,
    lengths,
    norm_gain,
    input_weight,
    gate_weight,
    decay_rate,
    frequency,
    log_step,
    input_map,
    readout_map,
    skip_weight,
    out_weight,
    state,
):
    own_seqs = state.shape[1]
    block_seqs, new_count, feature_count = tokens.shape
    all_seqs = lengths.shape[0]
    inner_width = input_weight.shape[2]
    dp_index = lax.axis_index("dp")
    tp_index = lax.axis_index("tp")
    dp_size = lax.axis_size("dp")
    tp_size = lax.axis_size("tp")
    positions = lax.broadcasted_iota(jnp.int32, (all_seqs, new_count), 1)
    alive_all = (positions < lengths[:, None]).astype(jnp.float32)
    alive_own = lax.dynamic_slice_in_dim(alive_all, dp_index * own_seqs, own_seqs, 0)
    own_rows = own_seqs * new_count
    block_count = block_seqs * new_count
    states = []
    gathered = gather_rows(tokens.reshape(block_count, feature_count), "tp", tp_size)
    for layer_index in range(LAYERS):
        flattened = gathered.astype(jnp.float32)
        scaled = (flattened * norm_gain[layer_index][None, :]).astype(jnp.bfloat16)
        partial_squares = jnp.sum(flattened * flattened, axis=1)
        part_drive = jnp.dot(scaled, input_weight[layer_index], preferred_element_type=jnp.float32)
        part_gate = jnp.dot(scaled, gate_weight[layer_index], preferred_element_type=jnp.float32)
        summed_drive, summed_gate, own_squares = scatter_projections(
            part_drive, part_gate, partial_squares, "dp", dp_size
        )
        inverse = lax.rsqrt(own_squares / D + epsilon)[:, None]
        drive_value = (
            (inverse * summed_drive).astype(jnp.bfloat16).reshape(own_seqs, new_count, inner_width)
        )
        gate_value = (
            (inverse * summed_gate).astype(jnp.bfloat16).reshape(own_seqs, new_count, inner_width)
        )
        next_state, branch = advance_state(
            drive_value,
            gate_value,
            state[layer_index],
            alive_own,
            decay_rate[layer_index],
            frequency[layer_index],
            log_step[layer_index],
            input_map[layer_index],
            readout_map[layer_index],
            skip_weight[layer_index],
        )
        states.append(next_state)
        weight_now = out_weight[layer_index]
        projected = jnp.dot(
            gather_rows(branch.reshape(own_rows, inner_width), "dp", dp_size),
            weight_now,
            preferred_element_type=jnp.float32,
        ).astype(jnp.bfloat16)
        last = layer_index == LAYERS - 1
        if direct(tp_size) and not last:
            parts = [projected] + [swap(projected, "tp", k, tp_size) for k in range(1, tp_size)]
            total = sum(part.astype(jnp.float32) for part in parts)
            gathered = (flattened + total).astype(jnp.bfloat16)
            continue
        if direct(tp_size):
            parts = exchange_rows(projected, "tp", tp_size)
            branch_sum = sum(part.astype(jnp.float32) for part in parts)
        else:
            branch_sum = lax.psum_scatter(
                projected, "tp", scatter_dimension=0, tiled=True
            ).astype(jnp.float32)
        own_base = lax.dynamic_slice_in_dim(flattened, tp_index * block_count, block_count, 0)
        own_block = (own_base + branch_sum).astype(jnp.bfloat16)
        if not last:
            gathered = lax.all_gather(own_block, "tp", axis=0, tiled=True)
    own_block = own_block.reshape(tokens.shape)
    return (own_block, jnp.stack(states))


LANES = 128
COST = 40000000000
SUBLANES = 8
VMEM = pl.BlockSpec(memory_space=pltpu.VMEM)
HBM = pl.BlockSpec(memory_space=pltpu.MemorySpace.HBM)


def vmem_call(kernel, outs, *operands, in_specs=None, scratch=(), limit=8 << 20, cost=0):
    outs = [jax.ShapeDtypeStruct(shape, dtype) for shape, dtype in outs]
    in_specs = in_specs or [VMEM] * len(operands)
    operands = [
        pltpu.with_memory_space_constraint(operand, pltpu.MemorySpace.HBM) if spec is HBM else operand
        for spec, operand in zip(in_specs, operands)
    ]
    return pl.pallas_call(
        kernel,
        out_shape=outs,
        in_specs=in_specs,
        out_specs=[VMEM] * len(outs),
        scratch_shapes=list(scratch),
        compiler_params=pltpu.CompilerParams(vmem_limit_bytes=limit),
        cost_estimate=pl.CostEstimate(flops=cost, bytes_accessed=0, transcendentals=0) if cost else None,
    )(*operands)


def twice(value):
    return jnp.concatenate([value, value], axis=-1)


def halves(value):
    high = value.astype(jnp.bfloat16)
    low = (value - high.astype(jnp.float32)).astype(jnp.bfloat16)
    return high, low


def group_mask():
    lane = lax.broadcasted_iota(jnp.int32, (SUBLANES, LANES), 1)
    row = lax.broadcasted_iota(jnp.int32, (SUBLANES, LANES), 0)
    return lane // S5_IN == row


def start_copies(sources, targets, semaphores):
    copies = [
        pltpu.make_async_copy(source, target, semaphores.at[i])
        for i, (source, target) in enumerate(zip(sources, targets))
    ]
    for copy in copies:
        copy.start()
    return copies


def wait_copies(copies):
    for copy in copies:
        copy.wait()


def parameter_step(
    decay, frequency, log_step, map_ref, readout_ref, real_ref, imag_ref, coupled_ref, seen_ref
):
    half, groups = decay.shape
    step = jnp.exp(log_step)
    magnitude = jnp.exp(-decay * step)
    angle = frequency * step
    real = magnitude * jnp.cos(angle)
    imag = magnitude * jnp.sin(angle)
    denominator = decay * decay + frequency * frequency
    coeff_real = (imag * frequency - (real - 1.0) * decay) / denominator
    coeff_imag = (-imag * decay - (real - 1.0) * frequency) / denominator

    def across(first, second):
        return jnp.transpose(jnp.concatenate([first, second], axis=0))

    real_ref[...] = across(real, real)
    imag_ref[...] = across(-imag, imag)
    scale_real = across(coeff_real, coeff_real)
    scale_imag = across(-coeff_imag, coeff_imag)
    upper = lax.broadcasted_iota(jnp.int32, (LANES, LANES), 0) < half
    for chunk in range(groups // SUBLANES):
        rows = slice(chunk * SUBLANES, (chunk + 1) * SUBLANES)
        values = map_ref[rows].astype(jnp.float32).reshape(LANES, LANES)
        spread = [
            jnp.broadcast_to(s[rows][:, None, :], (SUBLANES, S5_IN, LANES)).reshape(LANES, LANES)
            for s in (scale_real, scale_imag)
        ]
        coupled = spread[0] * values + spread[1] * pltpu.roll(values, half, 1)
        high, low = halves(coupled)
        coupled_ref[chunk, :LANES] = high
        coupled_ref[chunk, LANES:] = low
        seen = jnp.transpose(readout_ref[rows].astype(jnp.float32).reshape(LANES, LANES))
        seen_ref[chunk] = jnp.where(upper, seen, -seen).astype(jnp.bfloat16)


def mark_row(marks_ref, index):
    return jnp.broadcast_to(marks_ref[index : index + 1], (SUBLANES, LANES))


def parameter_kernel(
    layer, rows, decay_ref, frequency_ref, log_step_ref, map_ref, readout_ref, marks_ref, *refs
):
    state_refs, (real_ref, imag_ref, coupled_ref, seen_ref, carried_ref) = refs[:-5], refs[-5:]
    parameter_step(
        decay_ref[layer], frequency_ref[layer], log_step_ref[layer : layer + 1],
        map_ref.at[layer], readout_ref.at[layer], real_ref, imag_ref, coupled_ref, seen_ref,
    )
    groups = real_ref.shape[0]
    for chunk in range(groups // SUBLANES):
        at = slice(chunk * SUBLANES, (chunk + 1) * SUBLANES)
        real, imag = real_ref[at], imag_ref[at]
        decayed = []
        for state_ref in state_refs:
            value = state_ref[layer, at].astype(jnp.float32)
            decayed.append(real * value + imag * pltpu.roll(value, LANES // 2, 1))
        for r in range(rows):
            carried_ref[r, at] = sum(
                jnp.where(mark_row(marks_ref, k * rows + r) > 0.5, value, 0.0)
                for k, value in enumerate(decayed)
            )


def prepare(layer, rows, decay, frequency, log_step, input_map, readout_map, marks, states):
    groups = decay.shape[2]
    chunks = groups // SUBLANES
    return vmem_call(
        functools.partial(parameter_kernel, layer, rows),
        [((groups, LANES), jnp.float32)] * 2
        + [((chunks, size, LANES), jnp.bfloat16) for size in (2 * LANES, LANES)]
        + [((rows, groups, LANES), jnp.float32)],
        decay, frequency, log_step, input_map, readout_map, marks, *states,
        cost=COST,
    )


def narrow_kernel(state_ref, out_ref):
    out_ref[...] = state_ref[...].astype(jnp.bfloat16)


def small_kernel(size, steps, lengths_hbm, *refs):
    count = (len(refs) - 5) // 2
    sources, targets = refs[:count], refs[count : 2 * count]
    pick_ref, spread_ref, marks_ref, lengths, semaphores = refs[2 * count :]
    copies = start_copies([lengths_hbm, *sources], [lengths, *targets], semaphores)
    copies[0].wait()
    dp_index, tp_index = lax.axis_index("dp"), lax.axis_index("tp")
    rows = pick_ref.shape[0]
    length = [lengths[s] for s in range(size)]
    offset = [sum(length[:s], 0 * length[0]) for s in range(size)]

    def of(values, index):
        return sum(jnp.where(index == s, values[s], 0) for s in range(size))

    def places(shape):
        return [lax.broadcasted_iota(jnp.int32, shape, axis) for axis in (0, 1)]

    row, lane = places((rows, LANES))
    chosen = jnp.zeros((rows, LANES), jnp.float32)
    for s in range(size):
        t = lane - s * steps
        hit = (t >= 0) & (t < length[s]) & (row == offset[s] + t)
        chosen = jnp.where(hit, 1.0, chosen)
    pick_ref[...] = chosen.astype(jnp.bfloat16)
    row, lane = places((size * steps, LANES))
    chosen = jnp.zeros((size * steps, LANES), jnp.float32)
    for k in range(size):
        t = row - k * steps
        start, live = of(offset, tp_index ^ k), of(length, tp_index ^ k)
        hit = (t >= 0) & (t < live) & (lane == start + t)
        chosen = jnp.where(hit, 1.0, chosen)
    spread_ref[...] = chosen.astype(jnp.bfloat16)
    row, _ = places((rows, LANES))
    for k in range(size):
        marks_ref[k * rows : (k + 1) * rows] = (row == of(offset, dp_index ^ k)).astype(jnp.float32)
    fresh = row == offset[0]
    for s in range(1, size):
        fresh = fresh | (row == offset[s])
    marks_ref[size * rows : (size + 1) * rows] = jnp.where(fresh, 0.0, 1.0)
    last = of(offset, dp_index) + of(length, dp_index) - 1
    marks_ref[(size + 1) * rows :] = (row == last).astype(jnp.float32)
    wait_copies(copies[1:])


def bring_small(size, steps, rows, lengths, *arrays):
    return vmem_call(
        functools.partial(small_kernel, size, steps),
        [(a.shape, a.dtype) for a in arrays]
        + [((rows, LANES), jnp.bfloat16), ((size * steps, LANES), jnp.bfloat16)]
        + [(((size + 2) * rows, LANES), jnp.float32)],
        lengths, *arrays,
        in_specs=[HBM] * (1 + len(arrays)),
        scratch=[
            pltpu.SMEM(lengths.shape, jnp.int32),
            pltpu.SemaphoreType.DMA((1 + len(arrays),)),
        ],
        cost=COST,
    )


def far_swaps(value, axis, size):
    received = {}
    for k in range(2, size, 2):
        received[k] = swap(value, axis, k, size)
    return received


def swaps(values, axis, size):
    received = {}
    for k in reversed(range(1, size)):
        value = values[k] if isinstance(values, (list, tuple)) else values
        received[k] = swap(value, axis, k, size)
    return [received[k] for k in range(1, size)]


def project(layer, rows, gain_ref, drive_weight_ref, gate_weight_ref, message_ref):
    width = drive_weight_ref.shape[2]
    scaled = (rows * gain_ref[layer : layer + 1]).astype(jnp.bfloat16)
    squares = jnp.sum(rows * rows, axis=1, keepdims=True)
    lane = lax.broadcasted_iota(jnp.int32, (rows.shape[0], LANES), 1)
    extra = jnp.zeros((rows.shape[0], LANES), jnp.float32)
    for place in range(3):
        piece = squares.astype(jnp.bfloat16).astype(jnp.float32)
        extra = jnp.where(lane == place, piece, extra)
        squares = squares - piece
    message_ref[:, 2 * width :] = extra.astype(jnp.bfloat16)
    step = min(width, 512)
    for base, weight_ref in ((0, drive_weight_ref), (width, gate_weight_ref)):
        for at in range(0, width, step):
            value = jnp.dot(
                scaled, weight_ref[layer, :, at : at + step], preferred_element_type=jnp.float32
            )
            message_ref[:, base + at : base + at + step] = value.astype(jnp.bfloat16)


def pick(blocks, offset):
    bit = 1
    while bit < len(blocks):
        on = (offset & bit) != 0
        blocks = [jnp.where(on, blocks[k ^ bit], blocks[k]) for k in range(len(blocks))]
        bit *= 2
    return blocks


def first_kernel(size, pick_ref, *refs):
    block_refs, (gain_ref, drive_ref, gate_ref) = refs[:size], refs[size : size + 3]
    message_ref, rows_ref = refs[size + 3 :]
    blocks = [ref[...].astype(jnp.float32) for ref in block_refs]
    blocks = jnp.concatenate(pick(blocks, lax.axis_index("tp")), axis=0).astype(jnp.bfloat16)
    chosen = pick_ref[:, : blocks.shape[0]]
    rows = jnp.dot(chosen, blocks, preferred_element_type=jnp.float32)
    rows_ref[...] = rows
    project(0, rows, gain_ref, drive_ref, gate_ref, message_ref)


def next_kernel(size, layer, base_ref, *refs):
    part_refs, (gain_ref, drive_ref, gate_ref) = refs[:size], refs[size : size + 3]
    message_ref, rows_ref = refs[size + 3 :]
    rows = base_ref[...] + sum(ref[...].astype(jnp.float32) for ref in part_refs)
    rows = rows.astype(jnp.bfloat16).astype(jnp.float32)
    rows_ref[...] = rows
    project(layer, rows, gain_ref, drive_ref, gate_ref, message_ref)


def advance(size, layer, features, refs, next_ref, branch_ref):
    message_refs = refs[:size]
    marks_ref, real_ref, imag_ref, coupled_ref, seen_ref, carried_ref, skip_ref = refs[size:]
    rows, width = branch_ref.shape
    half = LANES // 2
    total = sum(ref[...].astype(jnp.float32) for ref in message_refs)
    squares = jnp.sum(total[:, 2 * width :], axis=1, keepdims=True)
    inverse = lax.rsqrt(squares / features + epsilon)
    drive = (inverse * total[:, :width]).astype(jnp.bfloat16).astype(jnp.float32)
    gate = (inverse * total[:, width : 2 * width]).astype(jnp.bfloat16).astype(jnp.float32)
    own_group = group_mask()
    goes_on = [mark_row(marks_ref, size * rows + r) for r in range(rows)]
    is_last = [mark_row(marks_ref, (size + 1) * rows + r) > 0.5 for r in range(rows)]
    tiles = [slice(r * SUBLANES, (r + 1) * SUBLANES) for r in range(rows)]
    for chunk in range(width // LANES):
        at = slice(chunk * LANES, (chunk + 1) * LANES)
        groups = slice(chunk * SUBLANES, (chunk + 1) * SUBLANES)
        fed = jnp.concatenate(
            [
                jnp.where(own_group, jnp.broadcast_to(drive[r : r + 1, at], (SUBLANES, LANES)), 0.0)
                for r in range(rows)
            ],
            axis=0,
        ).astype(jnp.bfloat16)
        pushed = jnp.dot(twice(fed), coupled_ref[chunk], preferred_element_type=jnp.float32)
        real, imag = real_ref[groups], imag_ref[groups]
        value = other = final = jnp.zeros((SUBLANES, LANES), jnp.float32)
        history = []
        for r in range(rows):
            entering = pushed[tiles[r]] + carried_ref[r, groups]
            turned = pltpu.roll(entering, half, 1)
            value, other = (
                goes_on[r] * (real * value + imag * other) + entering,
                goes_on[r] * (real * other - imag * value) + turned,
            )
            history.append(value)
            final = jnp.where(is_last[r], value, final)
        next_ref[groups] = final
        high, low = halves(jnp.concatenate(history, axis=0))
        seen = jnp.dot(
            jnp.concatenate([high, low], axis=0), seen_ref[chunk], preferred_element_type=jnp.float32
        )
        seen = seen[: rows * SUBLANES] + seen[rows * SUBLANES :]
        read = jnp.concatenate(
            [jnp.sum(jnp.where(own_group, seen[tile], 0.0), axis=0, keepdims=True) for tile in tiles],
            axis=0,
        )
        response = read + skip_ref[layer : layer + 1, at].astype(jnp.float32) * drive[:, at]
        result = jax.nn.gelu(response) * jax.nn.silu(gate[:, at])
        branch_ref[:, at] = result.astype(jnp.bfloat16)


def state_kernel(size, layer, features, *refs):
    part_ref, next_ref, branch_ref = refs[-3:]
    advance(size, layer, features, refs[:-4], next_ref, branch_ref)
    part_ref[...] = jnp.dot(
        branch_ref[...], refs[-4][layer], preferred_element_type=jnp.float32
    ).astype(jnp.bfloat16)


def last_state_kernel(size, layer, features, *refs):
    ahead = len(refs) - (size + 2)
    spread_ref, base_ref, own_ref, weight_ref = refs[ahead - 4 : ahead]
    out_refs, (next_ref, branch_ref) = refs[ahead:-2], refs[-2:]
    advance(size, layer, features, refs[: ahead - 4], next_ref, branch_ref)
    part = jnp.dot(branch_ref[...], weight_ref[layer], preferred_element_type=jnp.float32)
    steps = own_ref.shape[0]
    spread = spread_ref[:, : 2 * part.shape[0]]

    def place(chosen, rows):
        rows = jnp.concatenate([rows, jnp.zeros_like(rows)], axis=0).astype(jnp.bfloat16)
        return jnp.dot(chosen, rows, preferred_element_type=jnp.float32)

    placed = place(spread, part)
    base = place(spread, base_ref[...])[:steps]
    live = jnp.sum(spread[:steps].astype(jnp.float32), axis=1, keepdims=True)
    base = base + jnp.where(live > 0.5, 0.0, own_ref[...].astype(jnp.float32))
    out_refs[0][...] = base + placed[:steps]
    for k in range(1, size):
        out_refs[k][...] = placed[k * steps : (k + 1) * steps].astype(jnp.bfloat16)


def final_kernel(own_ref, *refs):
    total = own_ref[...] + sum(ref[...].astype(jnp.float32) for ref in refs[:-1])
    refs[-1][0] = total.astype(jnp.bfloat16)


def fits(tokens, lengths, state, map_rows, dp_size, tp_size):
    whole_groups = state.shape[2] % LANES == 0 and state.shape[3] == LANES
    one_each = tokens.shape[0] == 1 and state.shape[1] == 1
    equal = dp_size == tp_size == lengths.shape[0]
    one_tile = 2 * lengths.shape[0] == SUBLANES
    whole_maps = one_tile and whole_groups and map_rows == S5_IN
    return direct(dp_size) and equal and one_each and whole_maps


def direct_steps(
    tokens,
    lengths,
    norm_gain,
    input_weight,
    gate_weight,
    decay_rate,
    frequency,
    log_step,
    input_map,
    readout_map,
    skip_weight,
    out_weight,
    state,
):
    size = lax.axis_size("dp")
    _, steps, features = tokens.shape
    inner = input_weight.shape[2]
    groups = state.shape[2]
    count = 2 * size
    bf16, f32 = jnp.bfloat16, jnp.float32
    decay, frequency = (jnp.swapaxes(value, 1, 2) for value in (decay_rate, frequency))
    raw = (decay, frequency, log_step, input_map, readout_map)
    wide = state.reshape(LAYERS, groups, LANES)
    own, gain, chosen, spread, marks = bring_small(
        size, steps, count, lengths, tokens.reshape(steps, features), norm_gain
    )
    pieces = [own] + swaps(own, "tp", size)
    (narrow,) = vmem_call(narrow_kernel, [(wide.shape, bf16)], wide, cost=COST)
    carried = {0: wide}
    carried.update(far_swaps(narrow, "dp", size))
    weights = (gain, input_weight, gate_weight)
    states = []
    for layer in range(LAYERS):
        if layer == 0:
            kernel, base = functools.partial(first_kernel, size), [chosen]
        else:
            kernel, base = functools.partial(next_kernel, size, layer), [rows]
        message, rows = vmem_call(
            kernel,
            [((count, 2 * inner + LANES), bf16), ((count, features), f32)],
            *base, *pieces, *weights,
        )
        arrived = [message] + swaps(message, "dp", size)
        if layer == 0:
            near = [0] + [k for k in range(2, size, 2)]
            for k in near:
                carried[k + 1] = swap(carried[k] if k else narrow, "dp", 1, size)
        fixed = prepare(layer, count, *raw, marks, [carried[k] for k in range(size)])
        operands = [*arrived, marks, *fixed, skip_weight]
        last = layer == LAYERS - 1
        outs = [((groups, LANES), f32)]
        scratch = [pltpu.VMEM((count, inner), bf16)]
        if not last:
            part, next_state = vmem_call(
                functools.partial(state_kernel, size, layer, D),
                [((count, features), bf16)] + outs,
                *operands, out_weight, scratch=scratch,
            )
            states.append(next_state)
            pieces = [part] + swaps(part, "tp", size)
            continue
        *parts, next_state = vmem_call(
            functools.partial(last_state_kernel, size, layer, D),
            [((steps, features), f32)] + [((steps, features), bf16)] * (size - 1) + outs,
            *operands, spread, rows, own, out_weight, scratch=scratch,
        )
        states.append(next_state)
        arrived = swaps(parts, "tp", size)
        (mixed,) = vmem_call(final_kernel, [((1, steps, features), bf16)], parts[0], *arrived)
    return mixed, jnp.stack(states)[:, None]


def body(*arguments):
    tokens, lengths, input_map, state = (arguments[i] for i in (0, 1, 8, 12))
    sizes = lax.axis_size("dp"), lax.axis_size("tp")
    if fits(tokens, lengths, state, input_map.shape[2], *sizes):
        return direct_steps(*arguments)
    return general_body(*arguments)


def solution(mesh):
    step = jax.shard_map(
        body,
        mesh=mesh,
        in_specs=(
            P(("grp", "tp"), None, "dp"),
            P("grp"),
            P(None, "dp"),
            P(None, "dp", "tp"),
            P(None, "dp", "tp"),
            P(None, "tp", None),
            P(None, "tp", None),
            P(None, "tp"),
            P(None, "tp", None, None),
            P(None, "tp", None, None),
            P(None, "tp"),
            P(None, "tp", "dp"),
            P(None, ("grp", "dp"), "tp", None),
        ),
        out_specs=(P(("grp", "tp"), None, "dp"), P(None, ("grp", "dp"), "tp", None)),
        check_vma=False,
    )
    size = mesh.shape["dp"]
    if size != mesh.shape["tp"] or not direct(size):
        return step
    return step
```

```python
import functools

import jax
import jax.numpy as jnp
from jax import lax
from jax.experimental import pallas as pl
from jax.experimental.pallas import tpu as pltpu
from jax.sharding import PartitionSpec as P


D = 4096
S5_IN = 16
LAYERS = 2


epsilon = 1e-06


def advance_state(
    drive_value,
    gate_value,
    carried,
    alive_mask,
    decay_rate,
    frequency,
    log_step,
    input_map,
    readout_map,
    skip_row,
):
    seq_count, new_count, inner_width = drive_value.shape
    group_count = inner_width // S5_IN
    state_half = carried.shape[-1] // 2
    step_size = jnp.exp(log_step)[:, None]
    magnitude = jnp.exp(-decay_rate * step_size)
    turn_angle = frequency * step_size
    decay_real = magnitude * jnp.cos(turn_angle)
    decay_imag = magnitude * jnp.sin(turn_angle)
    denominator = decay_rate * decay_rate + frequency * frequency
    coeff_real = (-(decay_real - 1.0) * decay_rate + decay_imag * frequency) / denominator
    coeff_imag = (-decay_imag * decay_rate - (decay_real - 1.0) * frequency) / denominator
    map_real = input_map[..., :state_half].astype(jnp.float32)
    map_imag = input_map[..., state_half:].astype(jnp.float32)
    coupled = jnp.concatenate(
        [
            coeff_real[:, None, :] * map_real - coeff_imag[:, None, :] * map_imag,
            coeff_real[:, None, :] * map_imag + coeff_imag[:, None, :] * map_real,
        ],
        axis=-1,
    )
    inputs = drive_value.astype(jnp.float32).reshape(seq_count, new_count, group_count, S5_IN)
    pushed = jnp.einsum("stgi,giq->stgq", inputs, coupled, precision=lax.Precision.HIGHEST)
    real_state = carried[..., :state_half]
    imag_state = carried[..., state_half:]
    history = []
    for position in range(new_count):
        keep = alive_mask[:, position][:, None, None] > 0.5
        next_real = (
            decay_real * real_state - decay_imag * imag_state + pushed[:, position, :, :state_half]
        )
        next_imag = (
            decay_real * imag_state + decay_imag * real_state + pushed[:, position, :, state_half:]
        )
        real_state = jnp.where(keep, next_real, real_state)
        imag_state = jnp.where(keep, next_imag, imag_state)
        history.append(jnp.concatenate([real_state, -imag_state], axis=-1))
    stacked = jnp.stack(history, axis=1)
    readout = jnp.einsum(
        "stgq,giq->stgi", stacked, readout_map.astype(jnp.float32), precision=lax.Precision.HIGHEST
    )
    readout = readout.reshape(seq_count, new_count, inner_width)
    response = readout + skip_row.astype(jnp.float32) * inputs.reshape(
        seq_count, new_count, inner_width
    )
    branch = (
        jax.nn.gelu(response) * jax.nn.silu(gate_value.astype(jnp.float32)) * alive_mask[:, :, None]
    )
    return (jnp.concatenate([real_state, imag_state], axis=-1), branch.astype(jnp.bfloat16))


def direct(size):
    return 1 < size <= 8 and size & (size - 1) == 0


def swap(value, axis, distance, size):
    return lax.ppermute(value, axis, [(i, i ^ distance) for i in range(size)])


def gather_rows(block, axis, size):
    if not direct(size):
        return lax.all_gather(block, axis, axis=0, tiled=True)
    index = lax.axis_index(axis)
    slots = jnp.stack([block] + [swap(block, axis, k, size) for k in range(1, size)])
    ordered = [lax.dynamic_index_in_dim(slots, index ^ s, 0, keepdims=False) for s in range(size)]
    return jnp.concatenate(ordered, axis=0)


def exchange_rows(value, axis, size):
    index = lax.axis_index(axis)
    rows = value.shape[0] // size
    blocks = [
        lax.dynamic_slice_in_dim(value, (index ^ k) * rows, rows, 0) for k in range(size)
    ]
    return [blocks[0]] + [swap(blocks[k], axis, k, size) for k in range(1, size)]


def split_three(value):
    pieces = []
    for _ in range(3):
        piece = lax.reduce_precision(value, 8, 7)
        pieces.append(piece.astype(jnp.bfloat16))
        value = value - piece
    return pieces


def scatter_projections(part_drive, part_gate, squares, axis, size):
    index = lax.axis_index(axis)
    width = part_drive.shape[1]
    rows = part_drive.shape[0] // size
    if not direct(size):
        total = lax.psum(squares, axis)
        own = lax.dynamic_slice_in_dim(total, index * rows, rows, 0)
        drive, gate = (
            lax.psum_scatter(
                part.astype(jnp.bfloat16), axis, scatter_dimension=0, tiled=True
            ).astype(jnp.float32)
            for part in (part_drive, part_gate)
        )
        return drive, gate, own
    extra = jnp.stack(split_three(squares), axis=1)
    extra = jnp.pad(extra, ((0, 0), (0, 128 - extra.shape[1])))
    message = jnp.concatenate(
        [part_drive.astype(jnp.bfloat16), part_gate.astype(jnp.bfloat16), extra], axis=1
    )
    total = sum(part.astype(jnp.float32) for part in exchange_rows(message, axis, size))
    own = jnp.sum(total[:, 2 * width :], axis=1)
    return total[:, :width], total[:, width : 2 * width], own


def general_body(
    tokens,
    lengths,
    norm_gain,
    input_weight,
    gate_weight,
    decay_rate,
    frequency,
    log_step,
    input_map,
    readout_map,
    skip_weight,
    out_weight,
    state,
):
    own_seqs = state.shape[1]
    block_seqs, new_count, feature_count = tokens.shape
    all_seqs = lengths.shape[0]
    inner_width = input_weight.shape[2]
    dp_index = lax.axis_index("dp")
    tp_index = lax.axis_index("tp")
    dp_size = lax.axis_size("dp")
    tp_size = lax.axis_size("tp")
    positions = lax.broadcasted_iota(jnp.int32, (all_seqs, new_count), 1)
    alive_all = (positions < lengths[:, None]).astype(jnp.float32)
    alive_own = lax.dynamic_slice_in_dim(alive_all, dp_index * own_seqs, own_seqs, 0)
    own_rows = own_seqs * new_count
    block_count = block_seqs * new_count
    states = []
    gathered = gather_rows(tokens.reshape(block_count, feature_count), "tp", tp_size)
    for layer_index in range(LAYERS):
        flattened = gathered.astype(jnp.float32)
        scaled = (flattened * norm_gain[layer_index][None, :]).astype(jnp.bfloat16)
        partial_squares = jnp.sum(flattened * flattened, axis=1)
        part_drive = jnp.dot(scaled, input_weight[layer_index], preferred_element_type=jnp.float32)
        part_gate = jnp.dot(scaled, gate_weight[layer_index], preferred_element_type=jnp.float32)
        summed_drive, summed_gate, own_squares = scatter_projections(
            part_drive, part_gate, partial_squares, "dp", dp_size
        )
        inverse = lax.rsqrt(own_squares / D + epsilon)[:, None]
        drive_value = (
            (inverse * summed_drive).astype(jnp.bfloat16).reshape(own_seqs, new_count, inner_width)
        )
        gate_value = (
            (inverse * summed_gate).astype(jnp.bfloat16).reshape(own_seqs, new_count, inner_width)
        )
        next_state, branch = advance_state(
            drive_value,
            gate_value,
            state[layer_index],
            alive_own,
            decay_rate[layer_index],
            frequency[layer_index],
            log_step[layer_index],
            input_map[layer_index],
            readout_map[layer_index],
            skip_weight[layer_index],
        )
        states.append(next_state)
        weight_now = out_weight[layer_index]
        projected = jnp.dot(
            gather_rows(branch.reshape(own_rows, inner_width), "dp", dp_size),
            weight_now,
            preferred_element_type=jnp.float32,
        ).astype(jnp.bfloat16)
        last = layer_index == LAYERS - 1
        if direct(tp_size) and not last:
            parts = [projected] + [swap(projected, "tp", k, tp_size) for k in range(1, tp_size)]
            total = sum(part.astype(jnp.float32) for part in parts)
            gathered = (flattened + total).astype(jnp.bfloat16)
            continue
        if direct(tp_size):
            parts = exchange_rows(projected, "tp", tp_size)
            branch_sum = sum(part.astype(jnp.float32) for part in parts)
        else:
            branch_sum = lax.psum_scatter(
                projected, "tp", scatter_dimension=0, tiled=True
            ).astype(jnp.float32)
        own_base = lax.dynamic_slice_in_dim(flattened, tp_index * block_count, block_count, 0)
        own_block = (own_base + branch_sum).astype(jnp.bfloat16)
        if not last:
            gathered = lax.all_gather(own_block, "tp", axis=0, tiled=True)
    own_block = own_block.reshape(tokens.shape)
    return (own_block, jnp.stack(states))


SMALL_COST = 4000000
LANES = 128
COST = 40000000000
SUBLANES = 8
VMEM = pl.BlockSpec(memory_space=pltpu.VMEM)
HBM = pl.BlockSpec(memory_space=pltpu.MemorySpace.HBM)


def vmem_call(kernel, outs, *operands, in_specs=None, scratch=(), limit=8 << 20, cost=0):
    outs = [jax.ShapeDtypeStruct(shape, dtype) for shape, dtype in outs]
    in_specs = in_specs or [VMEM] * len(operands)
    operands = [
        pltpu.with_memory_space_constraint(operand, pltpu.MemorySpace.HBM) if spec is HBM else operand
        for spec, operand in zip(in_specs, operands)
    ]
    return pl.pallas_call(
        kernel,
        out_shape=outs,
        in_specs=in_specs,
        out_specs=[VMEM] * len(outs),
        scratch_shapes=list(scratch),
        compiler_params=pltpu.CompilerParams(vmem_limit_bytes=limit),
        cost_estimate=pl.CostEstimate(flops=cost, bytes_accessed=0, transcendentals=0) if cost else None,
    )(*operands)


def twice(value):
    return jnp.concatenate([value, value], axis=-1)


def halves(value):
    high = value.astype(jnp.bfloat16)
    low = (value - high.astype(jnp.float32)).astype(jnp.bfloat16)
    return high, low


def group_mask():
    lane = lax.broadcasted_iota(jnp.int32, (SUBLANES, LANES), 1)
    row = lax.broadcasted_iota(jnp.int32, (SUBLANES, LANES), 0)
    return lane // S5_IN == row


def start_copies(sources, targets, semaphores):
    copies = [
        pltpu.make_async_copy(source, target, semaphores.at[i])
        for i, (source, target) in enumerate(zip(sources, targets))
    ]
    for copy in copies:
        copy.start()
    return copies


def wait_copies(copies):
    for copy in copies:
        copy.wait()


def parameter_step(
    decay, frequency, log_step, map_ref, readout_ref, real_ref, imag_ref, coupled_ref, seen_ref
):
    half, groups = decay.shape
    step = jnp.exp(log_step)
    magnitude = jnp.exp(-decay * step)
    angle = frequency * step
    real = magnitude * jnp.cos(angle)
    imag = magnitude * jnp.sin(angle)
    denominator = decay * decay + frequency * frequency
    coeff_real = (imag * frequency - (real - 1.0) * decay) / denominator
    coeff_imag = (-imag * decay - (real - 1.0) * frequency) / denominator

    def across(first, second):
        return jnp.transpose(jnp.concatenate([first, second], axis=0))

    real_ref[...] = across(real, real)
    imag_ref[...] = across(-imag, imag)
    scale_real = across(coeff_real, coeff_real)
    scale_imag = across(-coeff_imag, coeff_imag)
    upper = lax.broadcasted_iota(jnp.int32, (LANES, LANES), 0) < half
    for chunk in range(groups // SUBLANES):
        rows = slice(chunk * SUBLANES, (chunk + 1) * SUBLANES)
        values = map_ref[rows].astype(jnp.float32).reshape(LANES, LANES)
        spread = [
            jnp.broadcast_to(s[rows][:, None, :], (SUBLANES, S5_IN, LANES)).reshape(LANES, LANES)
            for s in (scale_real, scale_imag)
        ]
        coupled = spread[0] * values + spread[1] * pltpu.roll(values, half, 1)
        high, low = halves(coupled)
        coupled_ref[chunk, :LANES] = high
        coupled_ref[chunk, LANES:] = low
        seen = jnp.transpose(readout_ref[rows].astype(jnp.float32).reshape(LANES, LANES))
        seen_ref[chunk] = jnp.where(upper, seen, -seen).astype(jnp.bfloat16)


def mark_row(marks_ref, index):
    return jnp.broadcast_to(marks_ref[index : index + 1], (SUBLANES, LANES))


def parameter_kernel(
    layer, rows, decay_ref, frequency_ref, log_step_ref, map_ref, readout_ref, marks_ref, *refs
):
    state_refs, (real_ref, imag_ref, coupled_ref, seen_ref, carried_ref) = refs[:-5], refs[-5:]
    parameter_step(
        decay_ref[layer], frequency_ref[layer], log_step_ref[layer : layer + 1],
        map_ref.at[layer], readout_ref.at[layer], real_ref, imag_ref, coupled_ref, seen_ref,
    )
    groups = real_ref.shape[0]
    for chunk in range(groups // SUBLANES):
        at = slice(chunk * SUBLANES, (chunk + 1) * SUBLANES)
        real, imag = real_ref[at], imag_ref[at]
        decayed = []
        for state_ref in state_refs:
            value = state_ref[layer, at].astype(jnp.float32)
            decayed.append(real * value + imag * pltpu.roll(value, LANES // 2, 1))
        for r in range(rows):
            carried_ref[r, at] = sum(
                jnp.where(mark_row(marks_ref, k * rows + r) > 0.5, value, 0.0)
                for k, value in enumerate(decayed)
            )


def prepare(layer, rows, decay, frequency, log_step, input_map, readout_map, marks, states):
    groups = decay.shape[2]
    chunks = groups // SUBLANES
    return vmem_call(
        functools.partial(parameter_kernel, layer, rows),
        [((groups, LANES), jnp.float32)] * 2
        + [((chunks, size, LANES), jnp.bfloat16) for size in (2 * LANES, LANES)]
        + [((rows, groups, LANES), jnp.float32)],
        decay, frequency, log_step, input_map, readout_map, marks, *states,
        cost=SMALL_COST,
    )


def primer_kernel(out_ref):
    out_ref[...] = jnp.zeros_like(out_ref)


def narrow_kernel(state_ref, out_ref):
    out_ref[...] = state_ref[...].astype(jnp.bfloat16)


def small_kernel(size, steps, primer_ref, lengths_hbm, *refs):
    count = (len(refs) - 5) // 2
    sources, targets = refs[:count], refs[count : 2 * count]
    pick_ref, spread_ref, marks_ref, lengths, semaphores = refs[2 * count :]
    copies = start_copies([lengths_hbm, *sources], [lengths, *targets], semaphores)
    copies[0].wait()
    dp_index, tp_index = lax.axis_index("dp"), lax.axis_index("tp")
    rows = pick_ref.shape[0]
    length = [lengths[s] for s in range(size)]
    offset = [sum(length[:s], 0 * length[0]) for s in range(size)]

    def of(values, index):
        return sum(jnp.where(index == s, values[s], 0) for s in range(size))

    def places(shape):
        return [lax.broadcasted_iota(jnp.int32, shape, axis) for axis in (0, 1)]

    row, lane = places((rows, LANES))
    chosen = jnp.zeros((rows, LANES), jnp.float32)
    for k in range(size):
        t = lane - k * steps
        start, live = of(offset, tp_index ^ k), of(length, tp_index ^ k)
        hit = (t >= 0) & (t < live) & (row == start + t)
        chosen = jnp.where(hit, 1.0, chosen)
    pick_ref[...] = chosen.astype(jnp.bfloat16)
    row, lane = places((size * steps, LANES))
    chosen = jnp.zeros((size * steps, LANES), jnp.float32)
    for k in range(size):
        t = row - k * steps
        start, live = of(offset, tp_index ^ k), of(length, tp_index ^ k)
        hit = (t >= 0) & (t < live) & (lane == start + t)
        chosen = jnp.where(hit, 1.0, chosen)
    spread_ref[...] = chosen.astype(jnp.bfloat16)
    row, _ = places((rows, LANES))
    for k in range(size):
        marks_ref[k * rows : (k + 1) * rows] = (row == of(offset, dp_index ^ k)).astype(jnp.float32)
    fresh = row == offset[0]
    for s in range(1, size):
        fresh = fresh | (row == offset[s])
    marks_ref[size * rows : (size + 1) * rows] = jnp.where(fresh, 0.0, 1.0)
    last = of(offset, dp_index) + of(length, dp_index) - 1
    marks_ref[(size + 1) * rows :] = (row == last).astype(jnp.float32)
    wait_copies(copies[1:])


def bring_small(size, steps, rows, primer, lengths, *arrays):
    return vmem_call(
        functools.partial(small_kernel, size, steps),
        [(a.shape, a.dtype) for a in arrays]
        + [((rows, LANES), jnp.bfloat16), ((size * steps, LANES), jnp.bfloat16)]
        + [(((size + 2) * rows, LANES), jnp.float32)],
        primer, lengths, *arrays,
        in_specs=[VMEM] + [HBM] * (1 + len(arrays)),
        scratch=[
            pltpu.SMEM(lengths.shape, jnp.int32),
            pltpu.SemaphoreType.DMA((1 + len(arrays),)),
        ],
        cost=SMALL_COST,
    )


def far_swaps(value, axis, size):
    received = {}
    for k in range(3, size, 2):
        received[k] = swap(value, axis, k, size)
    return received


def swaps(values, axis, size):
    received = {}
    for k in reversed(range(1, size)):
        value = values[k] if isinstance(values, (list, tuple)) else values
        received[k] = swap(value, axis, k, size)
    return [received[k] for k in range(1, size)]


def project(layer, rows, gain_ref, drive_weight_ref, gate_weight_ref, message_ref):
    width = drive_weight_ref.shape[2]
    scaled = (rows * gain_ref[layer : layer + 1]).astype(jnp.bfloat16)
    squares = jnp.sum(rows * rows, axis=1, keepdims=True)
    lane = lax.broadcasted_iota(jnp.int32, (rows.shape[0], LANES), 1)
    extra = jnp.zeros((rows.shape[0], LANES), jnp.float32)
    for place in range(3):
        piece = squares.astype(jnp.bfloat16).astype(jnp.float32)
        extra = jnp.where(lane == place, piece, extra)
        squares = squares - piece
    message_ref[:, 2 * width :] = extra.astype(jnp.bfloat16)
    step = min(width, 512)
    for base, weight_ref in ((0, drive_weight_ref), (width, gate_weight_ref)):
        for at in range(0, width, step):
            value = jnp.dot(
                scaled, weight_ref[layer, :, at : at + step], preferred_element_type=jnp.float32
            )
            message_ref[:, base + at : base + at + step] = value.astype(jnp.bfloat16)


def first_kernel(size, pick_ref, *refs):
    block_refs, (gain_ref, drive_ref, gate_ref) = refs[:size], refs[size : size + 3]
    message_ref, rows_ref = refs[size + 3 :]
    blocks = [ref[...].astype(jnp.float32) for ref in block_refs]
    blocks = jnp.concatenate(blocks, axis=0).astype(jnp.bfloat16)
    chosen = pick_ref[:, : blocks.shape[0]]
    rows = jnp.dot(chosen, blocks, preferred_element_type=jnp.float32)
    rows_ref[...] = rows
    project(0, rows, gain_ref, drive_ref, gate_ref, message_ref)


def next_kernel(size, layer, base_ref, *refs):
    part_refs, (gain_ref, drive_ref, gate_ref) = refs[:size], refs[size : size + 3]
    message_ref, rows_ref = refs[size + 3 :]
    rows = base_ref[...] + sum(ref[...].astype(jnp.float32) for ref in part_refs)
    rows = rows.astype(jnp.bfloat16).astype(jnp.float32)
    rows_ref[...] = rows
    project(layer, rows, gain_ref, drive_ref, gate_ref, message_ref)


def advance(size, layer, features, refs, next_ref, branch_ref):
    message_refs = refs[:size]
    marks_ref, real_ref, imag_ref, coupled_ref, seen_ref, carried_ref, skip_ref = refs[size:]
    rows, width = branch_ref.shape
    half = LANES // 2
    total = sum(ref[...].astype(jnp.float32) for ref in message_refs)
    squares = jnp.sum(total[:, 2 * width :], axis=1, keepdims=True)
    inverse = lax.rsqrt(squares / features + epsilon)
    drive = (inverse * total[:, :width]).astype(jnp.bfloat16).astype(jnp.float32)
    gate = (inverse * total[:, width : 2 * width]).astype(jnp.bfloat16).astype(jnp.float32)
    own_group = group_mask()
    goes_on = [mark_row(marks_ref, size * rows + r) for r in range(rows)]
    is_last = [mark_row(marks_ref, (size + 1) * rows + r) > 0.5 for r in range(rows)]
    tiles = [slice(r * SUBLANES, (r + 1) * SUBLANES) for r in range(rows)]
    for chunk in range(width // LANES):
        at = slice(chunk * LANES, (chunk + 1) * LANES)
        groups = slice(chunk * SUBLANES, (chunk + 1) * SUBLANES)
        fed = jnp.concatenate(
            [
                jnp.where(own_group, jnp.broadcast_to(drive[r : r + 1, at], (SUBLANES, LANES)), 0.0)
                for r in range(rows)
            ],
            axis=0,
        ).astype(jnp.bfloat16)
        pushed = jnp.dot(twice(fed), coupled_ref[chunk], preferred_element_type=jnp.float32)
        real, imag = real_ref[groups], imag_ref[groups]
        value = other = final = jnp.zeros((SUBLANES, LANES), jnp.float32)
        history = []
        for r in range(rows):
            entering = pushed[tiles[r]] + carried_ref[r, groups]
            turned = pltpu.roll(entering, half, 1)
            value, other = (
                goes_on[r] * (real * value + imag * other) + entering,
                goes_on[r] * (real * other - imag * value) + turned,
            )
            history.append(value)
            final = jnp.where(is_last[r], value, final)
        next_ref[groups] = final
        high, low = halves(jnp.concatenate(history, axis=0))
        seen = jnp.dot(
            jnp.concatenate([high, low], axis=0), seen_ref[chunk], preferred_element_type=jnp.float32
        )
        seen = seen[: rows * SUBLANES] + seen[rows * SUBLANES :]
        read = jnp.concatenate(
            [jnp.sum(jnp.where(own_group, seen[tile], 0.0), axis=0, keepdims=True) for tile in tiles],
            axis=0,
        )
        response = read + skip_ref[layer : layer + 1, at].astype(jnp.float32) * drive[:, at]
        result = jax.nn.gelu(response) * jax.nn.silu(gate[:, at])
        branch_ref[:, at] = result.astype(jnp.bfloat16)


def state_kernel(size, layer, features, *refs):
    part_ref, next_ref, branch_ref = refs[-3:]
    advance(size, layer, features, refs[:-4], next_ref, branch_ref)
    part_ref[...] = jnp.dot(
        branch_ref[...], refs[-4][layer], preferred_element_type=jnp.float32
    ).astype(jnp.bfloat16)


def last_state_kernel(size, layer, features, *refs):
    ahead = len(refs) - (size + 2)
    spread_ref, base_ref, own_ref, weight_ref = refs[ahead - 4 : ahead]
    out_refs, (next_ref, branch_ref) = refs[ahead:-2], refs[-2:]
    advance(size, layer, features, refs[: ahead - 4], next_ref, branch_ref)
    part = jnp.dot(branch_ref[...], weight_ref[layer], preferred_element_type=jnp.float32)
    steps = own_ref.shape[0]
    spread = spread_ref[:, : 2 * part.shape[0]]

    def place(chosen, rows):
        rows = jnp.concatenate([rows, jnp.zeros_like(rows)], axis=0).astype(jnp.bfloat16)
        return jnp.dot(chosen, rows, preferred_element_type=jnp.float32)

    placed = place(spread, part)
    base = place(spread, base_ref[...])[:steps]
    live = jnp.sum(spread[:steps].astype(jnp.float32), axis=1, keepdims=True)
    base = base + jnp.where(live > 0.5, 0.0, own_ref[...].astype(jnp.float32))
    out_refs[0][...] = base + placed[:steps]
    for k in range(1, size):
        out_refs[k][...] = placed[k * steps : (k + 1) * steps].astype(jnp.bfloat16)


def final_kernel(own_ref, *refs):
    total = own_ref[...] + sum(ref[...].astype(jnp.float32) for ref in refs[:-1])
    refs[-1][0] = total.astype(jnp.bfloat16)


def fits(tokens, lengths, state, map_rows, dp_size, tp_size):
    whole_groups = state.shape[2] % LANES == 0 and state.shape[3] == LANES
    one_each = tokens.shape[0] == 1 and state.shape[1] == 1
    equal = dp_size == tp_size == lengths.shape[0]
    one_tile = 2 * lengths.shape[0] == SUBLANES
    whole_maps = one_tile and whole_groups and map_rows == S5_IN
    return direct(dp_size) and equal and one_each and whole_maps


def direct_steps(
    tokens,
    lengths,
    norm_gain,
    input_weight,
    gate_weight,
    decay_rate,
    frequency,
    log_step,
    input_map,
    readout_map,
    skip_weight,
    out_weight,
    state,
):
    size = lax.axis_size("dp")
    _, steps, features = tokens.shape
    inner = input_weight.shape[2]
    groups = state.shape[2]
    count = 2 * size
    bf16, f32 = jnp.bfloat16, jnp.float32
    decay, frequency = (jnp.swapaxes(value, 1, 2) for value in (decay_rate, frequency))
    raw = (decay, frequency, log_step, input_map, readout_map)
    wide = state.reshape(LAYERS, groups, LANES)
    (primer,) = vmem_call(primer_kernel, [((SUBLANES, LANES), f32)], cost=COST)
    own = tokens.reshape(steps, features)
    pieces = swaps(own, "tp", size)
    own, gain, chosen, spread, marks = bring_small(
        size, steps, count, primer, lengths, own, norm_gain
    )
    pieces = [own] + pieces
    (narrow,) = vmem_call(narrow_kernel, [(wide.shape, bf16)], wide, cost=SMALL_COST)
    carried = {0: wide}
    carried.update(far_swaps(narrow, "dp", size))
    weights = (gain, input_weight, gate_weight)
    states = []
    for layer in range(LAYERS):
        if layer == 0:
            kernel, base = functools.partial(first_kernel, size), [chosen]
        else:
            kernel, base = functools.partial(next_kernel, size, layer), [rows]
        message, rows = vmem_call(
            kernel,
            [((count, 2 * inner + LANES), bf16), ((count, features), f32)],
            *base, *pieces, *weights,
        )
        arrived = [message] + swaps(message, "dp", size)
        if layer == 0:
            for k in [0] + [k for k in range(3, size, 2)]:
                carried[k ^ 1] = swap(carried[k] if k else narrow, "dp", 1, size)
        fixed = prepare(layer, count, *raw, marks, [carried[k] for k in range(size)])
        operands = [*arrived, marks, *fixed, skip_weight]
        last = layer == LAYERS - 1
        outs = [((groups, LANES), f32)]
        scratch = [pltpu.VMEM((count, inner), bf16)]
        if not last:
            part, next_state = vmem_call(
                functools.partial(state_kernel, size, layer, D),
                [((count, features), bf16)] + outs,
                *operands, out_weight, scratch=scratch,
            )
            states.append(next_state)
            pieces = [part] + swaps(part, "tp", size)
            continue
        *parts, next_state = vmem_call(
            functools.partial(last_state_kernel, size, layer, D),
            [((steps, features), f32)] + [((steps, features), bf16)] * (size - 1) + outs,
            *operands, spread, rows, own, out_weight, scratch=scratch,
        )
        states.append(next_state)
        arrived = swaps(parts, "tp", size)
        (mixed,) = vmem_call(final_kernel, [((1, steps, features), bf16)], parts[0], *arrived)
    return mixed, jnp.stack(states)[:, None]


def body(*arguments):
    tokens, lengths, input_map, state = (arguments[i] for i in (0, 1, 8, 12))
    sizes = lax.axis_size("dp"), lax.axis_size("tp")
    if fits(tokens, lengths, state, input_map.shape[2], *sizes):
        return direct_steps(*arguments)
    return general_body(*arguments)


def solution(mesh):
    step = jax.shard_map(
        body,
        mesh=mesh,
        in_specs=(
            P(("grp", "tp"), None, "dp"),
            P("grp"),
            P(None, "dp"),
            P(None, "dp", "tp"),
            P(None, "dp", "tp"),
            P(None, "tp", None),
            P(None, "tp", None),
            P(None, "tp"),
            P(None, "tp", None, None),
            P(None, "tp", None, None),
            P(None, "tp"),
            P(None, "tp", "dp"),
            P(None, ("grp", "dp"), "tp", None),
        ),
        out_specs=(P(("grp", "tp"), None, "dp"), P(None, ("grp", "dp"), "tp", None)),
        check_vma=False,
    )
    size = mesh.shape["dp"]
    if size != mesh.shape["tp"] or not direct(size):
        return step
    return step
```

```python
import functools

import jax
import jax.numpy as jnp
from jax import lax
from jax.experimental import pallas as pl
from jax.experimental.pallas import tpu as pltpu
from jax.sharding import PartitionSpec as P


D = 4096
S5_IN = 16
LAYERS = 2


epsilon = 1e-06


def advance_state(
    drive_value,
    gate_value,
    carried,
    alive_mask,
    decay_rate,
    frequency,
    log_step,
    input_map,
    readout_map,
    skip_row,
):
    seq_count, new_count, inner_width = drive_value.shape
    group_count = inner_width // S5_IN
    state_half = carried.shape[-1] // 2
    step_size = jnp.exp(log_step)[:, None]
    magnitude = jnp.exp(-decay_rate * step_size)
    turn_angle = frequency * step_size
    decay_real = magnitude * jnp.cos(turn_angle)
    decay_imag = magnitude * jnp.sin(turn_angle)
    denominator = decay_rate * decay_rate + frequency * frequency
    coeff_real = (-(decay_real - 1.0) * decay_rate + decay_imag * frequency) / denominator
    coeff_imag = (-decay_imag * decay_rate - (decay_real - 1.0) * frequency) / denominator
    map_real = input_map[..., :state_half].astype(jnp.float32)
    map_imag = input_map[..., state_half:].astype(jnp.float32)
    coupled = jnp.concatenate(
        [
            coeff_real[:, None, :] * map_real - coeff_imag[:, None, :] * map_imag,
            coeff_real[:, None, :] * map_imag + coeff_imag[:, None, :] * map_real,
        ],
        axis=-1,
    )
    inputs = drive_value.astype(jnp.float32).reshape(seq_count, new_count, group_count, S5_IN)
    pushed = jnp.einsum("stgi,giq->stgq", inputs, coupled, precision=lax.Precision.HIGHEST)
    real_state = carried[..., :state_half]
    imag_state = carried[..., state_half:]
    history = []
    for position in range(new_count):
        keep = alive_mask[:, position][:, None, None] > 0.5
        next_real = (
            decay_real * real_state - decay_imag * imag_state + pushed[:, position, :, :state_half]
        )
        next_imag = (
            decay_real * imag_state + decay_imag * real_state + pushed[:, position, :, state_half:]
        )
        real_state = jnp.where(keep, next_real, real_state)
        imag_state = jnp.where(keep, next_imag, imag_state)
        history.append(jnp.concatenate([real_state, -imag_state], axis=-1))
    stacked = jnp.stack(history, axis=1)
    readout = jnp.einsum(
        "stgq,giq->stgi", stacked, readout_map.astype(jnp.float32), precision=lax.Precision.HIGHEST
    )
    readout = readout.reshape(seq_count, new_count, inner_width)
    response = readout + skip_row.astype(jnp.float32) * inputs.reshape(
        seq_count, new_count, inner_width
    )
    branch = (
        jax.nn.gelu(response) * jax.nn.silu(gate_value.astype(jnp.float32)) * alive_mask[:, :, None]
    )
    return (jnp.concatenate([real_state, imag_state], axis=-1), branch.astype(jnp.bfloat16))


def direct(size):
    return 1 < size <= 8 and size & (size - 1) == 0


def swap(value, axis, distance, size):
    return lax.ppermute(value, axis, [(i, i ^ distance) for i in range(size)])


def gather_rows(block, axis, size):
    if not direct(size):
        return lax.all_gather(block, axis, axis=0, tiled=True)
    index = lax.axis_index(axis)
    slots = jnp.stack([block] + [swap(block, axis, k, size) for k in range(1, size)])
    ordered = [lax.dynamic_index_in_dim(slots, index ^ s, 0, keepdims=False) for s in range(size)]
    return jnp.concatenate(ordered, axis=0)


def exchange_rows(value, axis, size):
    index = lax.axis_index(axis)
    rows = value.shape[0] // size
    blocks = [
        lax.dynamic_slice_in_dim(value, (index ^ k) * rows, rows, 0) for k in range(size)
    ]
    return [blocks[0]] + [swap(blocks[k], axis, k, size) for k in range(1, size)]


def split_three(value):
    pieces = []
    for _ in range(3):
        piece = lax.reduce_precision(value, 8, 7)
        pieces.append(piece.astype(jnp.bfloat16))
        value = value - piece
    return pieces


def scatter_projections(part_drive, part_gate, squares, axis, size):
    index = lax.axis_index(axis)
    width = part_drive.shape[1]
    rows = part_drive.shape[0] // size
    if not direct(size):
        total = lax.psum(squares, axis)
        own = lax.dynamic_slice_in_dim(total, index * rows, rows, 0)
        drive, gate = (
            lax.psum_scatter(
                part.astype(jnp.bfloat16), axis, scatter_dimension=0, tiled=True
            ).astype(jnp.float32)
            for part in (part_drive, part_gate)
        )
        return drive, gate, own
    extra = jnp.stack(split_three(squares), axis=1)
    extra = jnp.pad(extra, ((0, 0), (0, 128 - extra.shape[1])))
    message = jnp.concatenate(
        [part_drive.astype(jnp.bfloat16), part_gate.astype(jnp.bfloat16), extra], axis=1
    )
    total = sum(part.astype(jnp.float32) for part in exchange_rows(message, axis, size))
    own = jnp.sum(total[:, 2 * width :], axis=1)
    return total[:, :width], total[:, width : 2 * width], own


def general_body(
    tokens,
    lengths,
    norm_gain,
    input_weight,
    gate_weight,
    decay_rate,
    frequency,
    log_step,
    input_map,
    readout_map,
    skip_weight,
    out_weight,
    state,
):
    own_seqs = state.shape[1]
    block_seqs, new_count, feature_count = tokens.shape
    all_seqs = lengths.shape[0]
    inner_width = input_weight.shape[2]
    dp_index = lax.axis_index("dp")
    tp_index = lax.axis_index("tp")
    dp_size = lax.axis_size("dp")
    tp_size = lax.axis_size("tp")
    positions = lax.broadcasted_iota(jnp.int32, (all_seqs, new_count), 1)
    alive_all = (positions < lengths[:, None]).astype(jnp.float32)
    alive_own = lax.dynamic_slice_in_dim(alive_all, dp_index * own_seqs, own_seqs, 0)
    own_rows = own_seqs * new_count
    block_count = block_seqs * new_count
    states = []
    gathered = gather_rows(tokens.reshape(block_count, feature_count), "tp", tp_size)
    for layer_index in range(LAYERS):
        flattened = gathered.astype(jnp.float32)
        scaled = (flattened * norm_gain[layer_index][None, :]).astype(jnp.bfloat16)
        partial_squares = jnp.sum(flattened * flattened, axis=1)
        part_drive = jnp.dot(scaled, input_weight[layer_index], preferred_element_type=jnp.float32)
        part_gate = jnp.dot(scaled, gate_weight[layer_index], preferred_element_type=jnp.float32)
        summed_drive, summed_gate, own_squares = scatter_projections(
            part_drive, part_gate, partial_squares, "dp", dp_size
        )
        inverse = lax.rsqrt(own_squares / D + epsilon)[:, None]
        drive_value = (
            (inverse * summed_drive).astype(jnp.bfloat16).reshape(own_seqs, new_count, inner_width)
        )
        gate_value = (
            (inverse * summed_gate).astype(jnp.bfloat16).reshape(own_seqs, new_count, inner_width)
        )
        next_state, branch = advance_state(
            drive_value,
            gate_value,
            state[layer_index],
            alive_own,
            decay_rate[layer_index],
            frequency[layer_index],
            log_step[layer_index],
            input_map[layer_index],
            readout_map[layer_index],
            skip_weight[layer_index],
        )
        states.append(next_state)
        weight_now = out_weight[layer_index]
        projected = jnp.dot(
            gather_rows(branch.reshape(own_rows, inner_width), "dp", dp_size),
            weight_now,
            preferred_element_type=jnp.float32,
        ).astype(jnp.bfloat16)
        last = layer_index == LAYERS - 1
        if direct(tp_size) and not last:
            parts = [projected] + [swap(projected, "tp", k, tp_size) for k in range(1, tp_size)]
            total = sum(part.astype(jnp.float32) for part in parts)
            gathered = (flattened + total).astype(jnp.bfloat16)
            continue
        if direct(tp_size):
            parts = exchange_rows(projected, "tp", tp_size)
            branch_sum = sum(part.astype(jnp.float32) for part in parts)
        else:
            branch_sum = lax.psum_scatter(
                projected, "tp", scatter_dimension=0, tiled=True
            ).astype(jnp.float32)
        own_base = lax.dynamic_slice_in_dim(flattened, tp_index * block_count, block_count, 0)
        own_block = (own_base + branch_sum).astype(jnp.bfloat16)
        if not last:
            gathered = lax.all_gather(own_block, "tp", axis=0, tiled=True)
    own_block = own_block.reshape(tokens.shape)
    return (own_block, jnp.stack(states))


SMALL_COST = 4000000
LANES = 128
COST = 40000000000
SUBLANES = 8
VMEM = pl.BlockSpec(memory_space=pltpu.VMEM)
HBM = pl.BlockSpec(memory_space=pltpu.MemorySpace.HBM)


def vmem_call(kernel, outs, *operands, in_specs=None, scratch=(), limit=8 << 20, cost=0):
    outs = [jax.ShapeDtypeStruct(shape, dtype) for shape, dtype in outs]
    in_specs = in_specs or [VMEM] * len(operands)
    operands = [
        pltpu.with_memory_space_constraint(operand, pltpu.MemorySpace.HBM) if spec is HBM else operand
        for spec, operand in zip(in_specs, operands)
    ]
    return pl.pallas_call(
        kernel,
        out_shape=outs,
        in_specs=in_specs,
        out_specs=[VMEM] * len(outs),
        scratch_shapes=list(scratch),
        compiler_params=pltpu.CompilerParams(vmem_limit_bytes=limit),
        cost_estimate=pl.CostEstimate(flops=cost, bytes_accessed=0, transcendentals=0) if cost else None,
    )(*operands)


def twice(value):
    return jnp.concatenate([value, value], axis=-1)


def halves(value):
    high = value.astype(jnp.bfloat16)
    low = (value - high.astype(jnp.float32)).astype(jnp.bfloat16)
    return high, low


def group_mask():
    lane = lax.broadcasted_iota(jnp.int32, (SUBLANES, LANES), 1)
    row = lax.broadcasted_iota(jnp.int32, (SUBLANES, LANES), 0)
    return lane // S5_IN == row


def start_copies(sources, targets, semaphores):
    copies = [
        pltpu.make_async_copy(source, target, semaphores.at[i])
        for i, (source, target) in enumerate(zip(sources, targets))
    ]
    for copy in copies:
        copy.start()
    return copies


def wait_copies(copies):
    for copy in copies:
        copy.wait()


def parameter_step(
    decay, frequency, log_step, map_ref, readout_ref, real_ref, imag_ref, coupled_ref, seen_ref
):
    half, groups = decay.shape
    step = jnp.exp(log_step)
    magnitude = jnp.exp(-decay * step)
    angle = frequency * step
    real = magnitude * jnp.cos(angle)
    imag = magnitude * jnp.sin(angle)
    denominator = decay * decay + frequency * frequency
    coeff_real = (imag * frequency - (real - 1.0) * decay) / denominator
    coeff_imag = (-imag * decay - (real - 1.0) * frequency) / denominator

    def across(first, second):
        return jnp.transpose(jnp.concatenate([first, second], axis=0))

    real_ref[...] = across(real, real)
    imag_ref[...] = across(-imag, imag)
    scale_real = across(coeff_real, coeff_real)
    scale_imag = across(-coeff_imag, coeff_imag)
    upper = lax.broadcasted_iota(jnp.int32, (LANES, LANES), 0) < half
    for chunk in range(groups // SUBLANES):
        rows = slice(chunk * SUBLANES, (chunk + 1) * SUBLANES)
        values = map_ref[rows].astype(jnp.float32).reshape(LANES, LANES)
        spread = [
            jnp.broadcast_to(s[rows][:, None, :], (SUBLANES, S5_IN, LANES)).reshape(LANES, LANES)
            for s in (scale_real, scale_imag)
        ]
        coupled = spread[0] * values + spread[1] * pltpu.roll(values, half, 1)
        high, low = halves(coupled)
        coupled_ref[chunk, :LANES] = high
        coupled_ref[chunk, LANES:] = low
        seen = jnp.transpose(readout_ref[rows].astype(jnp.float32).reshape(LANES, LANES))
        seen_ref[chunk] = jnp.where(upper, seen, -seen).astype(jnp.bfloat16)


def mark_row(marks_ref, index):
    return jnp.broadcast_to(marks_ref[index : index + 1], (SUBLANES, LANES))


def parameter_kernel(
    layer, rows, decay_ref, frequency_ref, log_step_ref, map_ref, readout_ref, marks_ref, *refs
):
    state_refs, (real_ref, imag_ref, coupled_ref, seen_ref, carried_ref) = refs[:-5], refs[-5:]
    parameter_step(
        decay_ref[layer], frequency_ref[layer], log_step_ref[layer : layer + 1],
        map_ref.at[layer], readout_ref.at[layer], real_ref, imag_ref, coupled_ref, seen_ref,
    )
    groups = real_ref.shape[0]
    for chunk in range(groups // SUBLANES):
        at = slice(chunk * SUBLANES, (chunk + 1) * SUBLANES)
        real, imag = real_ref[at], imag_ref[at]
        decayed = []
        for state_ref in state_refs:
            value = state_ref[layer, at].astype(jnp.float32)
            decayed.append(real * value + imag * pltpu.roll(value, LANES // 2, 1))
        for r in range(rows):
            carried_ref[r, at] = sum(
                jnp.where(mark_row(marks_ref, k * rows + r) > 0.5, value, 0.0)
                for k, value in enumerate(decayed)
            )


def prepare(layer, rows, decay, frequency, log_step, input_map, readout_map, marks, states):
    groups = decay.shape[2]
    chunks = groups // SUBLANES
    return vmem_call(
        functools.partial(parameter_kernel, layer, rows),
        [((groups, LANES), jnp.float32)] * 2
        + [((chunks, size, LANES), jnp.bfloat16) for size in (2 * LANES, LANES)]
        + [((rows, groups, LANES), jnp.float32)],
        decay, frequency, log_step, input_map, readout_map, marks, *states,
        cost=SMALL_COST,
    )


def primer_kernel(out_ref):
    out_ref[...] = jnp.zeros_like(out_ref)


def narrow_kernel(state_ref, out_ref):
    out_ref[...] = state_ref[...].astype(jnp.bfloat16)


def small_kernel(size, steps, primer_ref, lengths_hbm, *refs):
    count = (len(refs) - 5) // 2
    sources, targets = refs[:count], refs[count : 2 * count]
    pick_ref, spread_ref, marks_ref, lengths, semaphores = refs[2 * count :]
    copies = start_copies([lengths_hbm, *sources], [lengths, *targets], semaphores)
    copies[0].wait()
    dp_index, tp_index = lax.axis_index("dp"), lax.axis_index("tp")
    rows = pick_ref.shape[0]
    length = [lengths[s] for s in range(size)]
    offset = [sum(length[:s], 0 * length[0]) for s in range(size)]

    def of(values, index):
        return sum(jnp.where(index == s, values[s], 0) for s in range(size))

    def places(shape):
        return [lax.broadcasted_iota(jnp.int32, shape, axis) for axis in (0, 1)]

    row, lane = places((rows, LANES))
    chosen = jnp.zeros((rows, LANES), jnp.float32)
    for k in range(size):
        t = lane - k * steps
        start, live = of(offset, tp_index ^ k), of(length, tp_index ^ k)
        hit = (t >= 0) & (t < live) & (row == start + t)
        chosen = jnp.where(hit, 1.0, chosen)
    pick_ref[...] = chosen.astype(jnp.bfloat16)
    row, lane = places((size * steps, LANES))
    chosen = jnp.zeros((size * steps, LANES), jnp.float32)
    for k in range(size):
        t = row - k * steps
        start, live = of(offset, tp_index ^ k), of(length, tp_index ^ k)
        hit = (t >= 0) & (t < live) & (lane == start + t)
        chosen = jnp.where(hit, 1.0, chosen)
    spread_ref[...] = chosen.astype(jnp.bfloat16)
    row, _ = places((rows, LANES))
    for k in range(size):
        marks_ref[k * rows : (k + 1) * rows] = (row == of(offset, dp_index ^ k)).astype(jnp.float32)
    fresh = row == offset[0]
    for s in range(1, size):
        fresh = fresh | (row == offset[s])
    marks_ref[size * rows : (size + 1) * rows] = jnp.where(fresh, 0.0, 1.0)
    last = of(offset, dp_index) + of(length, dp_index) - 1
    marks_ref[(size + 1) * rows :] = (row == last).astype(jnp.float32)
    wait_copies(copies[1:])


def bring_small(size, steps, rows, primer, lengths, *arrays):
    return vmem_call(
        functools.partial(small_kernel, size, steps),
        [(a.shape, a.dtype) for a in arrays]
        + [((rows, LANES), jnp.bfloat16), ((size * steps, LANES), jnp.bfloat16)]
        + [(((size + 2) * rows, LANES), jnp.float32)],
        primer, lengths, *arrays,
        in_specs=[VMEM] + [HBM] * (1 + len(arrays)),
        scratch=[
            pltpu.SMEM(lengths.shape, jnp.int32),
            pltpu.SemaphoreType.DMA((1 + len(arrays),)),
        ],
        cost=SMALL_COST,
    )


def far_swaps(value, axis, size):
    received = {}
    for k in range(3, size, 2):
        received[k] = swap(value, axis, k, size)
    return received


def swaps(values, axis, size):
    received = {}
    for k in reversed(range(1, size)):
        value = values[k] if isinstance(values, (list, tuple)) else values
        received[k] = swap(value, axis, k, size)
    return [received[k] for k in range(1, size)]


def project(layer, rows, gain_ref, drive_weight_ref, gate_weight_ref, message_ref):
    width = drive_weight_ref.shape[2]
    scaled = (rows * gain_ref[layer : layer + 1]).astype(jnp.bfloat16)
    squares = jnp.sum(rows * rows, axis=1, keepdims=True)
    lane = lax.broadcasted_iota(jnp.int32, (rows.shape[0], LANES), 1)
    extra = jnp.zeros((rows.shape[0], LANES), jnp.float32)
    for place in range(3):
        piece = squares.astype(jnp.bfloat16).astype(jnp.float32)
        extra = jnp.where(lane == place, piece, extra)
        squares = squares - piece
    message_ref[:, 2 * width :] = extra.astype(jnp.bfloat16)
    step = min(width, 512)
    for base, weight_ref in ((0, drive_weight_ref), (width, gate_weight_ref)):
        for at in range(0, width, step):
            value = jnp.dot(
                scaled, weight_ref[layer, :, at : at + step], preferred_element_type=jnp.float32
            )
            message_ref[:, base + at : base + at + step] = value.astype(jnp.bfloat16)


def first_kernel(size, pick_ref, *refs):
    block_refs, (gain_ref, drive_ref, gate_ref) = refs[:size], refs[size : size + 3]
    message_ref, rows_ref = refs[size + 3 :]
    blocks = [ref[...].astype(jnp.float32) for ref in block_refs]
    blocks = jnp.concatenate(blocks, axis=0).astype(jnp.bfloat16)
    chosen = pick_ref[:, : blocks.shape[0]]
    rows = jnp.dot(chosen, blocks, preferred_element_type=jnp.float32)
    rows_ref[...] = rows
    project(0, rows, gain_ref, drive_ref, gate_ref, message_ref)


def next_kernel(size, layer, base_ref, *refs):
    part_refs, (gain_ref, drive_ref, gate_ref) = refs[:size], refs[size : size + 3]
    message_ref, rows_ref = refs[size + 3 :]
    rows = base_ref[...] + sum(ref[...].astype(jnp.float32) for ref in part_refs)
    rows = rows.astype(jnp.bfloat16).astype(jnp.float32)
    rows_ref[...] = rows
    project(layer, rows, gain_ref, drive_ref, gate_ref, message_ref)


def advance(size, layer, features, refs, next_ref, branch_ref):
    message_refs = refs[:size]
    marks_ref, real_ref, imag_ref, coupled_ref, seen_ref, carried_ref, skip_ref = refs[size:]
    rows, width = branch_ref.shape
    half = LANES // 2
    total = sum(ref[...].astype(jnp.float32) for ref in message_refs)
    squares = jnp.sum(total[:, 2 * width :], axis=1, keepdims=True)
    inverse = lax.rsqrt(squares / features + epsilon)
    drive = (inverse * total[:, :width]).astype(jnp.bfloat16).astype(jnp.float32)
    gate = (inverse * total[:, width : 2 * width]).astype(jnp.bfloat16).astype(jnp.float32)
    own_group = group_mask()
    goes_on = [mark_row(marks_ref, size * rows + r) for r in range(rows)]
    is_last = [mark_row(marks_ref, (size + 1) * rows + r) > 0.5 for r in range(rows)]
    tiles = [slice(r * SUBLANES, (r + 1) * SUBLANES) for r in range(rows)]
    for chunk in range(width // LANES):
        at = slice(chunk * LANES, (chunk + 1) * LANES)
        groups = slice(chunk * SUBLANES, (chunk + 1) * SUBLANES)
        fed = jnp.concatenate(
            [
                jnp.where(own_group, jnp.broadcast_to(drive[r : r + 1, at], (SUBLANES, LANES)), 0.0)
                for r in range(rows)
            ],
            axis=0,
        ).astype(jnp.bfloat16)
        pushed = jnp.dot(twice(fed), coupled_ref[chunk], preferred_element_type=jnp.float32)
        real, imag = real_ref[groups], imag_ref[groups]
        value = other = final = jnp.zeros((SUBLANES, LANES), jnp.float32)
        history = []
        for r in range(rows):
            entering = pushed[tiles[r]] + carried_ref[r, groups]
            turned = pltpu.roll(entering, half, 1)
            value, other = (
                goes_on[r] * (real * value + imag * other) + entering,
                goes_on[r] * (real * other - imag * value) + turned,
            )
            history.append(value)
            final = jnp.where(is_last[r], value, final)
        next_ref[groups] = final
        high, low = halves(jnp.concatenate(history, axis=0))
        seen = jnp.dot(
            jnp.concatenate([high, low], axis=0), seen_ref[chunk], preferred_element_type=jnp.float32
        )
        seen = seen[: rows * SUBLANES] + seen[rows * SUBLANES :]
        read = jnp.concatenate(
            [jnp.sum(jnp.where(own_group, seen[tile], 0.0), axis=0, keepdims=True) for tile in tiles],
            axis=0,
        )
        response = read + skip_ref[layer : layer + 1, at].astype(jnp.float32) * drive[:, at]
        result = jax.nn.gelu(response) * jax.nn.silu(gate[:, at])
        branch_ref[:, at] = result.astype(jnp.bfloat16)


def state_kernel(size, layer, features, *refs):
    part_ref, next_ref, branch_ref = refs[-3:]
    advance(size, layer, features, refs[:-4], next_ref, branch_ref)
    part_ref[...] = jnp.dot(
        branch_ref[...], refs[-4][layer], preferred_element_type=jnp.float32
    ).astype(jnp.bfloat16)


def place(spread_ref, rows):
    chosen = spread_ref[:, : 2 * rows.shape[0]]
    rows = jnp.concatenate([rows, jnp.zeros_like(rows)], axis=0).astype(jnp.bfloat16)
    return jnp.dot(chosen, rows, preferred_element_type=jnp.float32)


def base_kernel(spread_ref, rows_ref, own_ref, base_ref):
    steps, count = own_ref.shape[0], rows_ref.shape[0]
    base = place(spread_ref, rows_ref[...])[:steps]
    chosen = spread_ref[:steps, : 2 * count].astype(jnp.float32)
    live = jnp.sum(chosen, axis=1, keepdims=True)
    base_ref[...] = base + jnp.where(live > 0.5, 0.0, own_ref[...].astype(jnp.float32))


def last_state_kernel(size, layer, features, *refs):
    ahead = len(refs) - (size + 2)
    spread_ref, base_ref, weight_ref = refs[ahead - 3 : ahead]
    out_refs, (next_ref, branch_ref) = refs[ahead:-2], refs[-2:]
    advance(size, layer, features, refs[: ahead - 3], next_ref, branch_ref)
    part = jnp.dot(branch_ref[...], weight_ref[layer], preferred_element_type=jnp.float32)
    steps = base_ref.shape[0]
    placed = place(spread_ref, part)
    out_refs[0][...] = base_ref[...] + placed[:steps]
    for k in range(1, size):
        out_refs[k][...] = placed[k * steps : (k + 1) * steps].astype(jnp.bfloat16)


def final_kernel(own_ref, *refs):
    total = own_ref[...] + sum(ref[...].astype(jnp.float32) for ref in refs[:-1])
    refs[-1][0] = total.astype(jnp.bfloat16)


def fits(tokens, lengths, state, map_rows, dp_size, tp_size):
    whole_groups = state.shape[2] % LANES == 0 and state.shape[3] == LANES
    one_each = tokens.shape[0] == 1 and state.shape[1] == 1
    equal = dp_size == tp_size == lengths.shape[0]
    one_tile = 2 * lengths.shape[0] == SUBLANES
    whole_maps = one_tile and whole_groups and map_rows == S5_IN
    return direct(dp_size) and equal and one_each and whole_maps


def direct_steps(
    tokens,
    lengths,
    norm_gain,
    input_weight,
    gate_weight,
    decay_rate,
    frequency,
    log_step,
    input_map,
    readout_map,
    skip_weight,
    out_weight,
    state,
):
    size = lax.axis_size("dp")
    _, steps, features = tokens.shape
    inner = input_weight.shape[2]
    groups = state.shape[2]
    count = 2 * size
    bf16, f32 = jnp.bfloat16, jnp.float32
    decay, frequency = (jnp.swapaxes(value, 1, 2) for value in (decay_rate, frequency))
    raw = (decay, frequency, log_step, input_map, readout_map)
    wide = state.reshape(LAYERS, groups, LANES)
    (primer,) = vmem_call(primer_kernel, [((SUBLANES, LANES), f32)], cost=COST)
    own = tokens.reshape(steps, features)
    pieces = swaps(own, "tp", size)
    own, gain, chosen, spread, marks = bring_small(
        size, steps, count, primer, lengths, own, norm_gain
    )
    pieces = [own] + pieces
    (narrow,) = vmem_call(narrow_kernel, [(wide.shape, bf16)], wide, cost=SMALL_COST)
    carried = {0: wide}
    carried.update(far_swaps(narrow, "dp", size))
    weights = (gain, input_weight, gate_weight)
    states = []
    for layer in range(LAYERS):
        if layer == 0:
            kernel, base = functools.partial(first_kernel, size), [chosen]
        else:
            kernel, base = functools.partial(next_kernel, size, layer), [rows]
        message, rows = vmem_call(
            kernel,
            [((count, 2 * inner + LANES), bf16), ((count, features), f32)],
            *base, *pieces, *weights,
        )
        arrived = [message] + swaps(message, "dp", size)
        if layer == 0:
            for k in [0] + [k for k in range(3, size, 2)]:
                carried[k ^ 1] = swap(carried[k] if k else narrow, "dp", 1, size)
        fixed = prepare(layer, count, *raw, marks, [carried[k] for k in range(size)])
        operands = [*arrived, marks, *fixed, skip_weight]
        last = layer == LAYERS - 1
        if last:
            (base,) = vmem_call(
                base_kernel, [((steps, features), f32)], spread, rows, own, cost=SMALL_COST
            )
        outs = [((groups, LANES), f32)]
        scratch = [pltpu.VMEM((count, inner), bf16)]
        if not last:
            part, next_state = vmem_call(
                functools.partial(state_kernel, size, layer, D),
                [((count, features), bf16)] + outs,
                *operands, out_weight, scratch=scratch,
            )
            states.append(next_state)
            pieces = [part] + swaps(part, "tp", size)
            continue
        *parts, next_state = vmem_call(
            functools.partial(last_state_kernel, size, layer, D),
            [((steps, features), f32)] + [((steps, features), bf16)] * (size - 1) + outs,
            *operands, spread, base, out_weight, scratch=scratch,
        )
        states.append(next_state)
        arrived = swaps(parts, "tp", size)
        (mixed,) = vmem_call(final_kernel, [((1, steps, features), bf16)], parts[0], *arrived)
    return mixed, jnp.stack(states)[:, None]


def body(*arguments):
    tokens, lengths, input_map, state = (arguments[i] for i in (0, 1, 8, 12))
    sizes = lax.axis_size("dp"), lax.axis_size("tp")
    if fits(tokens, lengths, state, input_map.shape[2], *sizes):
        return direct_steps(*arguments)
    return general_body(*arguments)


def solution(mesh):
    step = jax.shard_map(
        body,
        mesh=mesh,
        in_specs=(
            P(("grp", "tp"), None, "dp"),
            P("grp"),
            P(None, "dp"),
            P(None, "dp", "tp"),
            P(None, "dp", "tp"),
            P(None, "tp", None),
            P(None, "tp", None),
            P(None, "tp"),
            P(None, "tp", None, None),
            P(None, "tp", None, None),
            P(None, "tp"),
            P(None, "tp", "dp"),
            P(None, ("grp", "dp"), "tp", None),
        ),
        out_specs=(P(("grp", "tp"), None, "dp"), P(None, ("grp", "dp"), "tp", None)),
        check_vma=False,
    )
    size = mesh.shape["dp"]
    if size != mesh.shape["tp"] or not direct(size):
        return step
    return step
```
